512 devices in a mesh: sp: 32 (over z, core), tp: 16 (over y, x).
Axes of the slice: x: 4, y: 4, z: 16, core: 2. Of those that a mesh axis runs over, the one named last changes fastest.
Arguments:
- mixer_in: bfloat16 [2048, 2048], P('sp', 'tp'), may hold values from -6 to 6
- residual: bfloat16 [2048, 2048], P('sp', 'tp')
- doc_ids: int32 [2048], P('sp'), may hold values from 0 to 7, never falling along the last dimension, each value on 1 to 1280 neighbouring positions
- log_step: float32 [2, 128], P(None, 'tp'), as said below
- log_extra: float32 [2048, 128], P('sp', 'tp'), as said below
- in_mix: float32 [2, 128, 16, 128], P(None, 'tp'), may hold values from -1.5 to 1.5
- read_mix: float32 [2, 128, 128, 16], P(None, 'tp'), may hold values from -0.5 to 0.5
- skip_gain: float32 [2048], P('tp'), may hold values from -4 to 4
- out_weight: bfloat16 [2048, 2048], P('tp'), may hold values from -0.1875 to 0.1875
- norm_gain: float32 [2048], P('tp'), may hold values from 0.1 to 1.9
- routes: int32 [2048, 2], P('sp'), may hold values from 0 to 31, all different within a row; in each aligned block of 64 rows (0 to 63, 64 to 127, ...) at most 5 rows name the same one
- route_weight: float32 [2048, 2], P('sp'), may hold values from 0.25 to 1
- switch_matrices: bfloat16 [32, 2048, 4096], P('sp', None, 'tp'), may hold values from -0.125 to 0.125
- up_weight: bfloat16 [32, 2048, 4096], P('sp', None, 'tp'), may hold values from -0.125 to 0.125
- down_weight: bfloat16 [32, 4096, 2048], P('sp', 'tp'), may hold values from -0.125 to 0.125
Outputs:
- layer_out: bfloat16 [2048, 2048], P('sp', 'tp')
The draws below stay inside these ranges and needn't reach their ends.
Inputs may be any that keep to these rules, and one draw needn't show every extreme that they name: In each aligned block of 64 rows no expert is named by more than 5 routes, a bound that some block reaches; each row names 2 different experts. `doc_ids`: document numbers never fall; each document is a run of positions and one has exactly 1280 positions. `log_step`: logarithms of positive step sizes. `log_extra`: every entry is at most zero.
All inputs are finite; a program needn't handle non-finite values.
Results may differ from the reference program's by a relative error of at most 0.014.
Values may be sent and summed in bfloat16 or wider, within the bound.
No kernel may reach another device: no remote copies, remote signals or barrier semaphores. Data moves between devices by JAX's collectives and lax.ppermute only.
A program may use at most 64 MiB of HBM per device.

```python
import math
import jax
import jax.numpy as jnp
import numpy as np
from jax import lax

D = 2048
CH = 16
STATE = 64
FFE = 4096
TOP = 2
TOK_DEV = 64
GROUPS = 128
TOKENS = 2048
EXPERTS = 32
CAP = 5
DOCS = 8
DOC_MOST = 1280
N_SP = 32
N_TP = 16


def draw_residual(key, part):
    keys = jax.random.split(jax.random.fold_in(key, 11), 3)
    row_scale = jnp.exp(jax.random.uniform(keys[1], (TOKENS, 1), jnp.float32, math.log(0.3), math.log(3.0)))
    rough = jnp.exp(jax.random.uniform(keys[2], (1, D), jnp.float32, math.log(0.7), math.log(1.4)))
    word_location = jnp.arange(D, dtype=jnp.float32)[None, :] / D
    base = jax.random.normal(keys[0], (TOKENS, D), jnp.float32)
    column = jnp.exp(math.log(3.0) * (word_location - 0.5)) * rough
    values = base * row_scale * column
    return values.astype(jnp.bfloat16)


def draw_log_step(key, part):
    keys = jax.random.split(jax.random.fold_in(key, 21), 3)
    fast_share = 0.5
    fast = jax.random.uniform(keys[0], (2, GROUPS), jnp.float32) < fast_share
    fast_log = jax.random.uniform(keys[1], (2, GROUPS), jnp.float32, math.log(0.02), math.log(0.07))
    slow_log = jax.random.uniform(keys[2], (2, GROUPS), jnp.float32, math.log(0.4), math.log(1.6)) - math.log(TOKENS)
    return jnp.where(fast, fast_log, slow_log).astype(jnp.float32)


def draw_log_extra(key, part):
    keys = jax.random.split(jax.random.fold_in(key, 31), 3)
    blocks = TOKENS // TOK_DEV
    rate = jnp.exp(jax.random.uniform(keys[0], (blocks, GROUPS), jnp.float32, math.log(0.1), math.log(1.0))) / TOKENS
    settled_regime = -jnp.repeat(rate, TOK_DEV, axis=0)
    bucket_places = jax.random.randint(keys[1], (2, GROUPS), 0, TOKENS)
    tier_count = jnp.log(jax.random.uniform(keys[2], (2, GROUPS), jnp.float32, 0.5, 0.8))
    word_location = jnp.arange(TOKENS, dtype=jnp.int32)[:, None]
    packet_clusters = jnp.where(word_location == bucket_places[0][None, :], tier_count[0][None, :], 0.0) + jnp.where(word_location == bucket_places[1][None, :], tier_count[1][None, :], 0.0)
    return (settled_regime + packet_clusters).astype(jnp.float32)


def raised(drawn, own_key, source, target, parts, factor):
    def block_of(position):
        return (jnp.arange(drawn.shape[position]) // (drawn.shape[position] // parts)).reshape((-1,) + (1,) * (drawn.ndim - 1 - position))

    near = jax.random.permutation(own_key, parts)[block_of(target)]
    far = (block_of(target) + parts // 2) % parts
    return jnp.where((block_of(source) == near) | (block_of(source) == far), factor * drawn, drawn)


def steps_of(key, shape, pieces, least, largest):
    def one(dim, blocks):
        steps = jax.random.uniform(jax.random.fold_in(jax.random.fold_in(key, 6), dim), (blocks,), jnp.float32, least / len(pieces), largest / len(pieces))
        return jnp.repeat(jnp.exp(steps), shape[dim] // blocks).reshape((-1,) + (1,) * (len(shape) - dim - 1))

    factor_of = one(*pieces[0])
    for cut in pieces[1:]:
        factor_of = factor_of * one(*cut)
    return factor_of


def length_profile(count, total, most, skew):
    portions = [(1 << 20) // math.isqrt(standing ** skew) + 1 for standing in range(2, count + 1)]
    spare, given = total - most - (count - 1), [1] * (count - 1)
    while spare > 0:
        movable = [i for i in range(count - 1) if given[i] < most]
        mass, remaining = sum([portions[i] for i in movable]), spare
        for i in movable:
            addition = min(most - given[i], max(1, remaining * portions[i] // mass), spare)
            given[i] = given[i] + addition
            spare = spare - addition
    return np.array([most] + given)


def ragged_sizes(rng, number_of, total, most, lean):
    if number_of == 2:
        one = jax.random.randint(rng, (), max(1, total - most), min(most, total - 1) + 1)
        return jnp.stack([one, total - one])
    lengths = jnp.asarray(length_profile(number_of, total, most, lean), jnp.int32)
    pairs = (number_of - 1) // 2
    giver, receiver = lengths[1:1 + 2 * pairs:2], lengths[2:2 + 2 * pairs:2]
    margin = jnp.minimum(giver - 1, most - receiver)
    shifted = jax.random.randint(jax.random.fold_in(rng, 1), (pairs,), 0, 1 << 20) % (margin + 1)
    lengths = lengths.at[1:1 + 2 * pairs:2].set(giver - shifted).at[2:2 + 2 * pairs:2].set(receiver + shifted)
    return lengths[jax.random.permutation(jax.random.fold_in(rng, 2), number_of)]


def routed_block(key, own, number, rows, count, top, limit, lean):
    order = jax.random.permutation(key, count)
    crowded, ordinary = shares(count, rows * top, limit, lean, True), shares(count, rows * top, limit, lean, False)
    places = jnp.arange(count)

    def named(tallies, offset_by):
        used = int((tallies > 0).sum())
        fixed = max(1, used // 4)
        moved = fixed + (places - fixed + offset_by * (used - fixed)) % max(1, count - fixed)
        return jnp.zeros((count,), jnp.int32).at[order[jnp.where(places < fixed, places, moved)]].set(jnp.asarray(tallies, jnp.int32))

    tallies = jnp.where(number % 4 == 0, named(crowded, number // 4), named(ordinary, number - number // 4 - 1))
    mixed = jax.random.permutation(jax.random.fold_in(own, 3), count)
    donor, taker = mixed[0:count // 2 * 2:2], mixed[1:count // 2 * 2:2]
    margin = jnp.minimum(tallies[donor] - 1, limit - tallies[taker]) // 2
    margin = jnp.where((donor == order[0]) | (taker == order[0]) | (tallies[taker] == 0), 0, jnp.maximum(margin, 0))
    moved = jax.random.randint(jax.random.fold_in(own, 4), (count // 2,), 0, 1 << 20) % (margin + 1)
    tallies = tallies.at[donor].add(-moved).at[taker].add(moved)
    members = jnp.searchsorted(jnp.cumsum(tallies), jnp.arange(rows * top), side="right").astype(jnp.int32)
    table = members.reshape(top, rows).T
    table = table[jax.random.permutation(jax.random.fold_in(own, 1), rows)]
    offset_by = jax.random.randint(jax.random.fold_in(own, 2), (rows, 1), 0, top)
    return jnp.take_along_axis(table, (jnp.arange(top)[None, :] + offset_by) % top, axis=1)


def shares(amount, total, limit, slope, full):
    portions = [(1 << 20) // math.isqrt(grade ** slope) + 1 for grade in range(1, amount + 1)]
    largest = limit if full else min(limit, max(-(-total // amount), total * portions[0] // sum(portions)))
    least = 1 if total - largest >= amount - 1 else 0
    counts, rest = [largest] + [least] * (amount - 1), total - largest - least * (amount - 1)
    while rest > 0:
        movable = [i for i in range(1, amount) if counts[i] < largest] or [i for i in range(1, amount) if counts[i] < limit]
        pool, left = sum([portions[i] for i in movable]), rest
        for i in movable:
            addition = min(limit - counts[i], max(1, left * portions[i] // pool), rest)
            counts[i] = counts[i] + addition
            rest = rest - addition
    return np.array(counts)


def normal_values(own_key, shape, deviation, limit, cuts=(), kind=jnp.bfloat16):
    array = jax.random.normal(own_key, shape, jnp.float32) * deviation
    if len(cuts) > 0:
        array = steps_of(own_key, shape, cuts, -0.22, 0.18) * array
    return jnp.clip(array, min=-limit, max=limit).astype(kind)


def noise_with(own_key, dims, width, bound, cuts, heavy, kind=jnp.bfloat16):
    array = width * jax.random.normal(own_key, dims, jnp.float32)
    if cuts:
        array = array * steps_of(own_key, dims, cuts, -0.22, 0.18)
    return jnp.clip(raised(array, jax.random.fold_in(own_key, 3), *heavy), -bound, bound).astype(kind)


def setup_inputs(seed: int = 0) -> dict:
    splits = jax.random.split(jax.random.key(seed), 16)
    mixer_in = normal_values(splits[0], (TOKENS, D), 1.0, 6.0, ((0, 32), (1, 16)))
    residual = draw_residual(jax.random.fold_in(splits[15], 71), 0)
    doc_ids = jnp.searchsorted(jnp.cumsum(ragged_sizes(splits[2], DOCS, TOKENS, DOC_MOST, 1)), jnp.arange(TOKENS), side="right").astype(jnp.int32)
    log_step = draw_log_step(jax.random.fold_in(splits[15], 71), 0)
    log_extra = draw_log_extra(jax.random.fold_in(splits[15], 71), 0)
    in_mix = normal_values(splits[5], (2, GROUPS, CH, 2 * STATE), CH ** -0.5, 1.5, ((1, 16),), jnp.float32)
    read_mix = normal_values(splits[6], (2, GROUPS, 2 * STATE, CH), (2 * STATE) ** -0.5, 0.5, ((1, 16),), jnp.float32)
    skip_gain = normal_values(splits[7], (D,), 1.0, 4.0, ((0, 16),), jnp.float32)
    out_weight = noise_with(splits[8], (D, D), D ** -0.5, 0.1875, ((0, 16),), (0, 1, 16, 2.0))
    norm_gain = jnp.clip(1.0 + 0.18 * jax.random.normal(splits[9], (D,), jnp.float32), 0.1, 1.9)
    routes_keys = jax.random.split(jax.random.fold_in(splits[10], 1), TOKENS // TOK_DEV)
    routes_turns = jax.random.permutation(jax.random.fold_in(splits[10], 3), TOKENS // TOK_DEV)
    routes = jax.vmap(lambda own, number: routed_block(jax.random.fold_in(splits[10], 2), own, number, TOK_DEV, EXPERTS, TOP, CAP, 1))(routes_keys, routes_turns).reshape((TOKENS, TOP))
    route_weight = jnp.clip(0.25 + 0.75 * jax.random.uniform(splits[11], (TOKENS, TOP), jnp.float32) ** steps_of(splits[11], (TOKENS, TOP), ((0, 32),), -0.2, 0.2), 0.25, 1.0)
    switch_matrices = normal_values(splits[12], (EXPERTS, D, FFE), D ** -0.5, 0.125, ((0, 32), (2, 16)))
    up_weight = normal_values(splits[13], (EXPERTS, D, FFE), D ** -0.5, 0.125, ((0, 32), (2, 16)))
    down_weight = noise_with(splits[14], (EXPERTS, FFE, D), FFE ** -0.5, 0.125, ((0, 32), (1, 16)), (1, 2, 16, 2.0))
    return dict(mixer_in=mixer_in, residual=residual, doc_ids=doc_ids, log_step=log_step, log_extra=log_extra, in_mix=in_mix, read_mix=read_mix, skip_gain=skip_gain, out_weight=out_weight, norm_gain=norm_gain, routes=routes, route_weight=route_weight, switch_matrices=switch_matrices, up_weight=up_weight, down_weight=down_weight)


epsilon = 1e-06
precise = lax.Precision.HIGHEST

def complex_product(former, latter):
    return (former[0] * latter[0] - former[1] * latter[1], former[0] * latter[1] + former[1] * latter[0])

def chain_join(earlier, latter):
    decay_pair = complex_product(latter[0], earlier[0])
    carried = complex_product(latter[0], earlier[1])
    return (decay_pair, (carried[0] + latter[1][0], carried[1] + latter[1][1]))

def block_terms(inputs, extra_block, keep, step_size, weights):
    states_count = weights.shape[2] // 2
    magnitude = jnp.exp(-0.5 * step_size[None, :] + extra_block) * keep[:, None]
    phase_angle = jnp.pi * jnp.arange(states_count, dtype=jnp.float32)[None, :] * step_size[:, None]
    decay_pair = (magnitude[:, :, None] * jnp.cos(phase_angle)[None], magnitude[:, :, None] * jnp.sin(phase_angle)[None])
    projected = jnp.einsum('tgh,ghq->tgq', inputs, weights, precision=precise)
    input_scale = jnp.sqrt(-jnp.expm1(-step_size))[None, :, None]
    source_input = (input_scale * projected[:, :, :states_count], input_scale * projected[:, :, states_count:])
    return (decay_pair, source_input)

def sweep(inputs, log_extra, seg_float, step_size, weights, read_weights, backward):
    states_count = weights.shape[2] // 2
    blocks = (inputs.reshape(N_SP, TOK_DEV, GROUPS, CH), log_extra.reshape(N_SP, TOK_DEV, GROUPS), seg_float.reshape(N_SP, TOK_DEV))

    def advance(carried, block):
        block_in, block_extra, block_seg = block
        state_pair, edge_seg = carried
        if backward:
            neighbour = jnp.concatenate([block_seg[1:], edge_seg])
        else:
            neighbour = jnp.concatenate([edge_seg, block_seg[:-1]])
        keep = (neighbour == block_seg).astype(jnp.float32)
        decay_pair, source_input = block_terms(block_in, block_extra, keep, step_size, weights)
        decay_run, local_states = lax.associative_scan(chain_join, (decay_pair, source_input), axis=0, reverse=backward)
        incoming = complex_product(decay_run, state_pair)
        states = (local_states[0] + incoming[0], local_states[1] + incoming[1])
        readout = jnp.einsum('tgq,gqh->tgh', jnp.concatenate([states[0], states[1]], axis=2), read_weights, precision=precise)
        if backward:
            new_carry = ((states[0][0], states[1][0]), block_seg[:1])
        else:
            new_carry = ((states[0][-1], states[1][-1]), block_seg[-1:])
        return (new_carry, readout)
    zeros_state = jnp.zeros((GROUPS, states_count), jnp.float32)
    opening_segment = seg_float[-1:] if backward else seg_float[:1]
    unused, readouts = lax.scan(advance, ((zeros_state, zeros_state), opening_segment), blocks, reverse=backward)
    return readouts.reshape(TOKENS, D)

def reference(mixer_in, residual, doc_ids, log_step, log_extra, in_mix, read_mix, skip_gain, out_weight, norm_gain, routes, route_weight, switch_matrices, up_weight, down_weight):
    inputs = mixer_in.astype(jnp.float32).reshape(TOKENS, GROUPS, CH)
    seg_float = doc_ids.astype(jnp.float32)
    step_size = jnp.exp(log_step)
    mixed = skip_gain[None, :] * mixer_in.astype(jnp.float32)
    for direction in range(2):
        mixed = mixed + sweep(inputs, log_extra, seg_float, step_size[direction], in_mix[direction], read_mix[direction], direction == 1)
    activated = jax.nn.gelu(mixed).astype(jnp.bfloat16)
    width_block = D // N_TP
    projected = jnp.zeros((TOKENS, D), jnp.float32)
    for part_index in range(N_TP):
        lower = part_index * width_block
        partial_sum = jnp.dot(activated[:, lower:lower + width_block], out_weight[lower:lower + width_block], preferred_element_type=jnp.float32)
        projected = projected + lax.optimization_barrier(partial_sum.astype(jnp.bfloat16)).astype(jnp.float32)
    stream = (residual.astype(jnp.float32) + projected).astype(jnp.bfloat16)
    stream_values = stream.astype(jnp.float32)
    normed = (stream_values * lax.rsqrt(lax.optimization_barrier(jnp.mean(stream_values * stream_values, axis=1, keepdims=True)) + epsilon) * norm_gain[None, :]).astype(jnp.bfloat16)
    flat_routes = routes.reshape(N_SP, TOK_DEV * TOP)
    onehot = (flat_routes[:, :, None] == jnp.arange(EXPERTS, dtype=jnp.int32)[None, None, :]).astype(jnp.int32)
    slot_rank = lax.optimization_barrier(jnp.sum((jnp.cumsum(onehot, axis=1) - 1) * onehot, axis=2))
    slot_global = jnp.arange(N_SP, dtype=jnp.int32)[:, None] * CAP + slot_rank
    token_ids = (jnp.arange(TOKENS * TOP, dtype=jnp.int32) // TOP).reshape(N_SP, TOK_DEV * TOP)
    table = jnp.zeros((EXPERTS, N_SP * CAP), jnp.int32).at[flat_routes, slot_global].set(token_ids)
    hidden_block = FFE // N_TP

    def expert_rows(packed):
        row_ids, gate_part, up_part, down_part = packed
        gathered = normed[row_ids]
        gate_acts = jnp.dot(gathered, gate_part, preferred_element_type=jnp.float32)
        up_acts = jnp.dot(gathered, up_part, preferred_element_type=jnp.float32)
        hidden = (jax.nn.silu(gate_acts) * up_acts).astype(jnp.bfloat16)
        totals = jnp.zeros((N_SP * CAP, D), jnp.float32)
        for part_index in range(N_TP):
            lower = part_index * hidden_block
            partial_sum = jnp.dot(hidden[:, lower:lower + hidden_block], down_part[lower:lower + hidden_block], preferred_element_type=jnp.float32)
            totals = totals + lax.optimization_barrier(partial_sum.astype(jnp.bfloat16)).astype(jnp.float32)
        return totals.astype(jnp.bfloat16)
    answer_entries = lax.map(expert_rows, (table, switch_matrices, up_weight, down_weight))
    picked = answer_entries[flat_routes.reshape(-1), slot_global.reshape(-1)].reshape(TOKENS, TOP, D)
    mixture = lax.optimization_barrier(jnp.sum(picked.astype(jnp.float32) * route_weight[:, :, None], axis=1))
    return (stream_values + mixture).astype(jnp.bfloat16)
```

```python
import jax
import jax.numpy as jnp
from jax import lax
from jax.experimental import pallas as pl
from jax.experimental.pallas import tpu as pltpu
from jax.sharding import Mesh
from jax.sharding import PartitionSpec as P

TP = ("tp_0", "tp_1")
INTERPRET = False

epsilon = 1e-06
f32 = jnp.float32
bf16 = jnp.bfloat16

BLOCKS = 32
PEERS = 16
ROWS = 64
GROUPS = 8
SLOTS = 5
PAD = 8
EROWS = BLOCKS * SLOTS
SENT = EROWS + 16

VMEM = pl.BlockSpec(memory_space=pltpu.VMEM)
SMEM = pl.BlockSpec(memory_space=pltpu.SMEM)


def call(body, in_specs, outs, scratch=()):
    return pl.pallas_call(
        body,
        in_specs=in_specs,
        out_specs=[VMEM] * len(outs),
        out_shape=[jax.ShapeDtypeStruct(shape, dtype) for shape, dtype in outs],
        scratch_shapes=[pltpu.VMEM(shape, dtype) for shape, dtype in scratch],
        interpret=INTERPRET,
    )


def iota(shape, dim):
    return lax.broadcasted_iota(jnp.int32, shape, dim)


def mm(a, b):
    return jnp.dot(a, b, preferred_element_type=f32)


def mm_across(a, b):
    return lax.dot_general(a, b, (((1,), (1,)), ((), ())), preferred_element_type=f32)


def halves_joined(first, second):
    left = iota((128, 128), 1) < 64
    return (
        jnp.where(left, first, pltpu.roll(second, 64, 1)),
        jnp.where(left, pltpu.roll(first, 64, 1), second),
    )


def steps_by_lane(log_step):
    eye = iota((GROUPS, GROUPS), 0) == iota((GROUPS, GROUPS), 1)
    step = jnp.exp(log_step)
    columns = [
        jnp.sum(
            jnp.where(eye, jnp.broadcast_to(step[k : k + 1, :], (GROUPS, GROUPS)), 0.0),
            axis=1,
            keepdims=True,
        )
        for k in range(2)
    ]
    return jnp.where(iota((GROUPS, 128), 1) < 64, columns[0], columns[1])


def one_minus_exp(x):
    series = jnp.ones_like(x)
    for n in range(9, 1, -1):
        series = 1.0 - x * (1.0 / n) * series
    return jnp.where(x < 0.5, x * series, 1.0 - jnp.exp(-x))


def sweep_body(
    me_ref, docs_ref, log_step_ref, log_extra_ref, x_ref, in_mix_ref,
    message_ref, real_ref, imag_ref, keep_ref, turn_ref,
    masked, source, magnitude,
):
    lane = iota((GROUPS, 128), 1)
    fwd = lane < 64
    step = steps_by_lane(log_step_ref[...])
    theta = (jnp.pi * (lane & 63).astype(f32)) * step
    cos, sin = jnp.cos(theta), jnp.sin(theta)
    turn_ref[0] = cos
    turn_ref[1] = sin
    scale = jnp.sqrt(one_minus_exp(step))
    wide = iota((ROWS, 128), 1)
    x = x_ref[...].astype(f32)
    for g in range(GROUPS):
        masked[pl.ds(g, ROWS, stride=GROUPS), :] = jnp.where(wide // 16 == g, x, 0.0)
    log_extra = log_extra_ref[...]
    loss = -0.5 * step
    for n in range(ROWS):
        extra = jnp.broadcast_to(log_extra[:, n : n + 1], (GROUPS, 128))
        magnitude[pl.ds(GROUPS * n, GROUPS), :] = jnp.exp(loss + extra)
    mix_real, mix_imag = halves_joined(in_mix_ref[0], in_mix_ref[1])
    rows = masked[...].astype(bf16)
    source[0] = mm(rows, mix_real.astype(bf16))
    source[1] = mm(rows, mix_imag.astype(bf16))
    real = jnp.zeros((GROUPS, 128), f32)
    imag = jnp.zeros((GROUPS, 128), f32)
    total = jnp.ones((GROUPS, 128), f32)
    for n in range(ROWS):
        r = ROWS - 1 - n
        here, there = pl.ds(GROUPS * n, GROUPS), pl.ds(GROUPS * r, GROUPS)
        keep = jnp.where(fwd, magnitude[here, :], magnitude[there, :])
        if n > 0:
            same_fwd = jnp.where(docs_ref[n] == docs_ref[n - 1], 1.0, 0.0)
            same_bwd = jnp.where(docs_ref[r] == docs_ref[r + 1], 1.0, 0.0)
            keep = keep * jnp.where(fwd, same_fwd, same_bwd)
        new_real = scale * jnp.where(fwd, source[0, here, :], source[0, there, :])
        new_imag = scale * jnp.where(fwd, source[1, here, :], source[1, there, :])
        keep_ref[n] = keep
        real_ref[n] = new_real
        imag_ref[n] = new_imag
        by_cos, by_sin = keep * cos, keep * sin
        real, imag = (
            (by_cos * real + new_real) - by_sin * imag,
            (by_sin * real + new_imag) + by_cos * imag,
        )
        total = total * keep
    crossed = pltpu.roll(total, 64, 1)
    high = crossed.astype(bf16).astype(f32)
    decay = jnp.where((lane & 32) == 0, high, crossed - high)
    first_doc = docs_ref[0].astype(f32)
    last_doc = docs_ref[ROWS - 1].astype(f32)
    to_later = jnp.concatenate(
        [jnp.where(fwd, real, decay), jnp.where(fwd, imag, last_doc)], axis=0
    ).astype(bf16)
    to_earlier = jnp.concatenate(
        [jnp.where(fwd, decay, real), jnp.where(fwd, first_doc, imag)], axis=0
    ).astype(bf16)
    me = me_ref[0]
    for i in range(BLOCKS):
        @pl.when(me < i)
        def _():
            message_ref[i] = to_later

        @pl.when(me >= i)
        def _():
            message_ref[i] = to_earlier


def mixer_body(
    me_ref, docs_ref, message_ref, real_ref, imag_ref, keep_ref, turn_ref,
    x_ref, read_mix_ref, skip_ref, out_weight_ref,
    partial_ref,
    states, read_out,
):
    lane = iota((GROUPS, 128), 1)
    fwd = lane < 64
    odd = (lane & 32) != 0
    me = me_ref[0]
    mine = jnp.where(fwd, docs_ref[0].astype(f32), docs_ref[ROWS - 1].astype(f32))
    cos, sin = turn_ref[0], turn_ref[1]
    block_cos, block_sin = cos, sin
    for _ in range(6):
        block_cos, block_sin = (
            block_cos * block_cos - block_sin * block_sin,
            2.0 * block_cos * block_sin,
        )
    real = jnp.zeros((GROUPS, 128), f32)
    imag = jnp.zeros((GROUPS, 128), f32)
    for n in range(BLOCKS - 1):
        r = BLOCKS - 1 - n
        one, two = message_ref[n].astype(f32), message_ref[r].astype(f32)
        decay = pltpu.roll(jnp.where(fwd, two[:GROUPS], one[:GROUPS]), 64, 1)
        decay = decay + jnp.where(odd, pltpu.roll(decay, 32, 1), pltpu.roll(decay, 96, 1))
        doc = pltpu.roll(jnp.where(fwd, two[GROUPS:], one[GROUPS:]), 64, 1)
        same = doc == mine
        new_real = jnp.where(same, jnp.where(fwd, one[:GROUPS], two[:GROUPS]), 0.0)
        new_imag = jnp.where(same, jnp.where(fwd, one[GROUPS:], two[GROUPS:]), 0.0)
        by_cos, by_sin = decay * block_cos, decay * block_sin
        passed = jnp.where(fwd, (n < me).astype(jnp.int32), (r > me).astype(jnp.int32)) > 0
        real, imag = (
            jnp.where(passed, (by_cos * real + new_real) - by_sin * imag, real),
            jnp.where(passed, (by_sin * real + new_imag) + by_cos * imag, imag),
        )
    for n in range(ROWS):
        r = ROWS - 1 - n
        here, there = pl.ds(GROUPS * n, GROUPS), pl.ds(GROUPS * r, GROUPS)
        keep = keep_ref[n]
        by_cos, by_sin = keep * cos, keep * sin
        real, imag = (
            (by_cos * real + real_ref[n]) - by_sin * imag,
            (by_sin * real + imag_ref[n]) + by_cos * imag,
        )
        states[0, here, 0:64] = real[:, 0:64]
        states[0, there, 64:128] = real[:, 64:128]
        states[1, here, 0:64] = imag[:, 0:64]
        states[1, there, 64:128] = imag[:, 64:128]
    read_real, read_imag = halves_joined(read_mix_ref[0], read_mix_ref[1])
    read_out[...] = mm_across(states[0].astype(bf16), read_real.astype(bf16)) + mm_across(
        states[1].astype(bf16), read_imag.astype(bf16)
    )
    wide = iota((ROWS, 128), 1)
    mixed = skip_ref[...] * x_ref[...].astype(f32)
    for g in range(GROUPS):
        mixed = mixed + jnp.where(
            wide // 16 == g, read_out[pl.ds(g, ROWS, stride=GROUPS), :], 0.0
        )
    activated = jax.nn.gelu(mixed).astype(bf16)
    partial = mm(activated, out_weight_ref[...]).astype(bf16)
    for j in range(PEERS):
        partial_ref[j] = partial[:, 128 * j : 128 * (j + 1)]


def column(row):
    eye = iota((ROWS, ROWS), 0) == iota((ROWS, ROWS), 1)
    return jnp.sum(jnp.where(eye, row, 0.0), axis=1, keepdims=True)


def slots_down(routes, k):
    before = iota((ROWS, ROWS), 1) < iota((ROWS, ROWS), 0)
    expert = column(routes[k : k + 1])
    met = (expert == routes[0:1]).astype(f32) + (expert == routes[1:2]).astype(f32)
    rank = jnp.sum(jnp.where(before, met, 0.0), axis=1, keepdims=True)
    return expert * PAD + rank


def slots_across(routes, k):
    before = iota((ROWS, ROWS), 0) < iota((ROWS, ROWS), 1)
    expert = routes[k : k + 1]
    met = (column(routes[0:1]) == expert).astype(f32) + (column(routes[1:2]) == expert).astype(f32)
    rank = jnp.sum(jnp.where(before, met, 0.0), axis=0, keepdims=True)
    return expert * PAD + rank


def stream_body(arrived_ref, residual_ref, routes_ref, stream_ref, outgoing_ref):
    total = residual_ref[...].astype(f32)
    projected = arrived_ref[0].astype(f32)
    for j in range(1, PEERS):
        projected = projected + arrived_ref[j].astype(f32)
    stream = (total + projected).astype(bf16)
    stream_ref[...] = stream
    routes = routes_ref[...].astype(f32)
    slot = iota((BLOCKS * PAD, ROWS), 0).astype(f32)
    placing = (slot == slots_across(routes, 0)).astype(f32) + (
        slot == slots_across(routes, 1)
    ).astype(f32)
    outgoing_ref[...] = mm(placing.astype(bf16), stream).astype(bf16)


def packed_rows(shape, packed_dim):
    packed, padded = iota(shape, packed_dim), iota(shape, 1 - packed_dim)
    block = padded // PAD
    slot = padded - block * PAD
    return ((slot < SLOTS) & (packed == block * SLOTS + slot)).astype(f32).astype(bf16)


def copies_body(arrived_ref, gain_ref, copies_ref):
    rows = mm(packed_rows((EROWS, BLOCKS * PAD), 0), arrived_ref[...]).astype(bf16)
    gain = gain_ref[...]
    high = gain.astype(bf16).astype(f32)
    middle = (gain - high).astype(bf16).astype(f32)
    low = gain - high - middle
    row = iota((16, 128), 0)
    gains = jnp.where(
        row == 0, high, jnp.where(row == 1, middle, jnp.where(row == 2, low, 0.0))
    ).astype(bf16)
    for j in range(PEERS):
        copies_ref[j, 0:EROWS, :] = rows
        copies_ref[j, EROWS:SENT, :] = gains


def expert_body(rows_ref, gate_ref, up_ref, down_ref, terms_ref, normed):
    squares = jnp.zeros((EROWS, 128), f32)
    for j in range(PEERS):
        piece = rows_ref[j, 0:EROWS, :].astype(f32)
        squares = squares + piece * piece
    mean = jnp.sum(squares, axis=1, keepdims=True) / (128 * PEERS)
    factor = lax.rsqrt(mean + epsilon)
    for j in range(PEERS):
        gains = rows_ref[j, EROWS:SENT, :].astype(f32)
        gain = gains[0:1] + gains[1:2] + gains[2:3]
        piece = rows_ref[j, 0:EROWS, :].astype(f32)
        normed[:, 128 * j : 128 * (j + 1)] = (piece * factor * gain).astype(bf16)
    rows = normed[...]
    gate = mm(rows, gate_ref[0])
    up = mm(rows, up_ref[0])
    hidden = (jax.nn.silu(gate) * up).astype(bf16)
    terms = mm(hidden, down_ref[0]).astype(bf16)
    for j in range(PEERS):
        terms_ref[j] = terms[:, 128 * j : 128 * (j + 1)]


def answer_body(terms_ref, answer_ref):
    total = terms_ref[0].astype(f32)
    for j in range(1, PEERS):
        total = total + terms_ref[j].astype(f32)
    answer_ref[...] = mm(packed_rows((BLOCKS * PAD, EROWS), 1), total.astype(bf16)).astype(bf16)


def mixture_body(returned_ref, stream_ref, routes_ref, weight_ref, out_ref):
    routes, returned = routes_ref[...].astype(f32), returned_ref[...]
    slot = iota((ROWS, BLOCKS * PAD), 1).astype(f32)
    mixture = jnp.zeros((ROWS, 128), f32)
    for k in range(2):
        pick = (slot == slots_down(routes, k)).astype(f32).astype(bf16)
        mixture = mixture + mm(pick, returned) * column(weight_ref[k : k + 1, :])
    out_ref[...] = (stream_ref[...].astype(f32) + mixture).astype(bf16)


def exchanged(pieces, axis):
    return lax.all_to_all(pieces, axis, 0, 0, tiled=True)


def shards(
    mixer_in,
    residual,
    doc_ids,
    log_step,
    log_extra,
    in_mix,
    read_mix,
    skip_gain,
    out_weight,
    norm_gain,
    routes,
    route_weight,
    switch_matrices,
    up_weight,
    down_weight,
):
    me = lax.axis_index("sp").reshape(1)
    tall = GROUPS * ROWS
    message, real, imag, keep, turn = call(
        sweep_body,
        [SMEM, SMEM, VMEM, VMEM, VMEM, VMEM],
        [
            ((BLOCKS, 16, 128), bf16),
            ((ROWS, GROUPS, 128), f32),
            ((ROWS, GROUPS, 128), f32),
            ((ROWS, GROUPS, 128), f32),
            ((2, GROUPS, 128), f32),
        ],
        [((tall, 128), f32), ((2, tall, 128), f32), ((tall, 128), f32)],
    )(me, doc_ids, log_step, log_extra.T, mixer_in, in_mix.reshape(2, 128, 128))
    messages = exchanged(message, "sp")
    (partial,) = call(
        mixer_body,
        [SMEM, SMEM] + [VMEM] * 9,
        [((PEERS, ROWS, 128), bf16)],
        [((2, tall, 128), f32), ((tall, 128), f32)],
    )(
        me, doc_ids, messages, real, imag, keep, turn,
        mixer_in, read_mix.swapaxes(2, 3).reshape(2, 128, 128), skip_gain.reshape(1, 128), out_weight,
    )
    shares = exchanged(partial, TP)
    stream, outgoing = call(
        stream_body,
        [VMEM] * 3,
        [((ROWS, 128), bf16), ((BLOCKS * PAD, 128), bf16)],
    )(shares, residual, routes.T)
    arrived = exchanged(outgoing.reshape(BLOCKS, PAD, 128), "sp").reshape(BLOCKS * PAD, 128)
    (copies,) = call(copies_body, [VMEM] * 2, [((PEERS, SENT, 128), bf16)])(
        arrived, norm_gain.reshape(1, 128)
    )
    (terms,) = call(
        expert_body,
        [VMEM] * 4,
        [((PEERS, EROWS, 128), bf16)],
        [((EROWS, 128 * PEERS), bf16)],
    )(exchanged(copies, TP), switch_matrices, up_weight, down_weight)
    (answer,) = call(answer_body, [VMEM], [((BLOCKS * PAD, 128), bf16)])(exchanged(terms, TP))
    returned = exchanged(answer.reshape(BLOCKS, PAD, 128), "sp").reshape(BLOCKS * PAD, 128)
    (out,) = call(mixture_body, [VMEM] * 4, [((ROWS, 128), bf16)])(
        returned, stream, routes.T, route_weight.T
    )
    return out


def solution(mesh):
    split = Mesh(mesh.devices.reshape(mesh.shape["sp"], 4, 4), ("sp", "tp_0", "tp_1"))
    in_specs = (
        P("sp", TP),
        P("sp", TP),
        P("sp"),
        P(None, TP),
        P("sp", TP),
        P(None, TP, None, None),
        P(None, TP, None, None),
        P(TP),
        P(TP, None),
        P(TP),
        P("sp", None),
        P("sp", None),
        P("sp", None, TP),
        P("sp", None, TP),
        P("sp", TP, None),
    )
    out_specs = P("sp", TP)
    return jax.shard_map(
        shards, mesh=split, in_specs=in_specs, out_specs=out_specs, check_vma=False
    )
```

```python
import jax
import jax.numpy as jnp
from jax import lax
from jax.experimental import pallas as pl
from jax.experimental.pallas import tpu as pltpu
from jax.sharding import Mesh
from jax.sharding import PartitionSpec as P

TP = ("tp_0", "tp_1")
INTERPRET = False

epsilon = 1e-06
f32 = jnp.float32
bf16 = jnp.bfloat16

BLOCKS = 32
PEERS = 16
ROWS = 64
GROUPS = 8
SLOTS = 5
PAD = 8
EROWS = BLOCKS * SLOTS
SENT = EROWS + 16

VMEM = pl.BlockSpec(memory_space=pltpu.VMEM)
SMEM = pl.BlockSpec(memory_space=pltpu.SMEM)


def near(x):
    return x if INTERPRET else pltpu.with_memory_space_constraint(x, pltpu.VMEM)


def call(body, in_specs, outs, scratch=(), last=False):
    kept = jax.ShapeDtypeStruct if INTERPRET or last else pltpu.VMEM
    return pl.pallas_call(
        body,
        in_specs=in_specs,
        out_specs=[VMEM] * len(outs),
        out_shape=[kept(shape, dtype) for shape, dtype in outs],
        scratch_shapes=[pltpu.VMEM(shape, dtype) for shape, dtype in scratch],
        compiler_params=pltpu.CompilerParams(vmem_limit_bytes=16 * 2**20),
        interpret=INTERPRET,
    )


def iota(shape, dim):
    return lax.broadcasted_iota(jnp.int32, shape, dim)


def mm(a, b):
    return jnp.dot(a, b, preferred_element_type=f32)


def mm_across(a, b):
    return lax.dot_general(a, b, (((1,), (1,)), ((), ())), preferred_element_type=f32)


def halves_joined(first, second):
    left = iota((128, 128), 1) < 64
    return (
        jnp.where(left, first, pltpu.roll(second, 64, 1)),
        jnp.where(left, pltpu.roll(first, 64, 1), second),
    )


def steps_by_lane(log_step):
    eye = iota((GROUPS, GROUPS), 0) == iota((GROUPS, GROUPS), 1)
    step = jnp.exp(log_step)
    columns = [
        jnp.sum(
            jnp.where(eye, jnp.broadcast_to(step[k : k + 1, :], (GROUPS, GROUPS)), 0.0),
            axis=1,
            keepdims=True,
        )
        for k in range(2)
    ]
    return jnp.where(iota((GROUPS, 128), 1) < 64, columns[0], columns[1])


def one_minus_exp(x):
    series = jnp.ones_like(x)
    for n in range(9, 1, -1):
        series = 1.0 - x * (1.0 / n) * series
    return jnp.where(x < 0.5, x * series, 1.0 - jnp.exp(-x))


def sweep_body(
    me_ref, docs_ref, log_step_ref, log_extra_ref, x_ref, in_mix_ref,
    message_ref, real_ref, imag_ref, keep_ref, turn_ref,
    masked, source, magnitude,
):
    lane = iota((GROUPS, 128), 1)
    fwd = lane < 64
    step = steps_by_lane(log_step_ref[...])
    theta = (jnp.pi * (lane & 63).astype(f32)) * step
    cos, sin = jnp.cos(theta), jnp.sin(theta)
    turn_ref[0] = cos
    turn_ref[1] = sin
    scale = jnp.sqrt(one_minus_exp(step))
    wide = iota((ROWS, 128), 1)
    x = x_ref[...].astype(f32)
    for g in range(GROUPS):
        masked[pl.ds(g, ROWS, stride=GROUPS), :] = jnp.where(wide // 16 == g, x, 0.0)
    log_extra = log_extra_ref[...]
    loss = -0.5 * step
    for n in range(ROWS):
        extra = jnp.broadcast_to(log_extra[:, n : n + 1], (GROUPS, 128))
        magnitude[pl.ds(GROUPS * n, GROUPS), :] = jnp.exp(loss + extra)
    mix_real, mix_imag = halves_joined(in_mix_ref[0], in_mix_ref[1])
    rows = masked[...].astype(bf16)
    source[0] = mm(rows, mix_real.astype(bf16))
    source[1] = mm(rows, mix_imag.astype(bf16))
    real = jnp.zeros((GROUPS, 128), f32)
    imag = jnp.zeros((GROUPS, 128), f32)
    total = jnp.ones((GROUPS, 128), f32)
    for n in range(ROWS):
        r = ROWS - 1 - n
        here, there = pl.ds(GROUPS * n, GROUPS), pl.ds(GROUPS * r, GROUPS)
        keep = jnp.where(fwd, magnitude[here, :], magnitude[there, :])
        if n > 0:
            same_fwd = jnp.where(docs_ref[n] == docs_ref[n - 1], 1.0, 0.0)
            same_bwd = jnp.where(docs_ref[r] == docs_ref[r + 1], 1.0, 0.0)
            keep = keep * jnp.where(fwd, same_fwd, same_bwd)
        new_real = scale * jnp.where(fwd, source[0, here, :], source[0, there, :])
        new_imag = scale * jnp.where(fwd, source[1, here, :], source[1, there, :])
        keep_ref[n] = keep
        real_ref[n] = new_real
        imag_ref[n] = new_imag
        by_cos, by_sin = keep * cos, keep * sin
        real, imag = (
            (by_cos * real + new_real) - by_sin * imag,
            (by_sin * real + new_imag) + by_cos * imag,
        )
        total = total * keep
    crossed = pltpu.roll(total, 64, 1)
    high = crossed.astype(bf16).astype(f32)
    decay = jnp.where((lane & 32) == 0, high, crossed - high)
    first_doc = docs_ref[0].astype(f32)
    last_doc = docs_ref[ROWS - 1].astype(f32)
    to_later = jnp.concatenate(
        [jnp.where(fwd, real, decay), jnp.where(fwd, imag, last_doc)], axis=0
    ).astype(bf16)
    to_earlier = jnp.concatenate(
        [jnp.where(fwd, decay, real), jnp.where(fwd, first_doc, imag)], axis=0
    ).astype(bf16)
    me = me_ref[0]
    for i in range(BLOCKS):
        @pl.when(me < i)
        def _():
            message_ref[i] = to_later

        @pl.when(me >= i)
        def _():
            message_ref[i] = to_earlier


def mixer_body(
    me_ref, docs_ref, message_ref, real_ref, imag_ref, keep_ref, turn_ref,
    x_ref, read_mix_ref, skip_ref, out_weight_ref,
    partial_ref,
    states, read_out,
):
    lane = iota((GROUPS, 128), 1)
    fwd = lane < 64
    odd = (lane & 32) != 0
    me = me_ref[0]
    mine = jnp.where(fwd, docs_ref[0].astype(f32), docs_ref[ROWS - 1].astype(f32))
    cos, sin = turn_ref[0], turn_ref[1]
    block_cos, block_sin = cos, sin
    for _ in range(6):
        block_cos, block_sin = (
            block_cos * block_cos - block_sin * block_sin,
            2.0 * block_cos * block_sin,
        )
    real = jnp.zeros((GROUPS, 128), f32)
    imag = jnp.zeros((GROUPS, 128), f32)
    for n in range(BLOCKS - 1):
        r = BLOCKS - 1 - n
        one, two = message_ref[n].astype(f32), message_ref[r].astype(f32)
        decay = pltpu.roll(jnp.where(fwd, two[:GROUPS], one[:GROUPS]), 64, 1)
        decay = decay + jnp.where(odd, pltpu.roll(decay, 32, 1), pltpu.roll(decay, 96, 1))
        doc = pltpu.roll(jnp.where(fwd, two[GROUPS:], one[GROUPS:]), 64, 1)
        same = doc == mine
        new_real = jnp.where(same, jnp.where(fwd, one[:GROUPS], two[:GROUPS]), 0.0)
        new_imag = jnp.where(same, jnp.where(fwd, one[GROUPS:], two[GROUPS:]), 0.0)
        by_cos, by_sin = decay * block_cos, decay * block_sin
        passed = jnp.where(fwd, (n < me).astype(jnp.int32), (r > me).astype(jnp.int32)) > 0
        real, imag = (
            jnp.where(passed, (by_cos * real + new_real) - by_sin * imag, real),
            jnp.where(passed, (by_sin * real + new_imag) + by_cos * imag, imag),
        )
    for n in range(ROWS):
        r = ROWS - 1 - n
        here, there = pl.ds(GROUPS * n, GROUPS), pl.ds(GROUPS * r, GROUPS)
        keep = keep_ref[n]
        by_cos, by_sin = keep * cos, keep * sin
        real, imag = (
            (by_cos * real + real_ref[n]) - by_sin * imag,
            (by_sin * real + imag_ref[n]) + by_cos * imag,
        )
        states[0, here, 0:64] = real[:, 0:64]
        states[0, there, 64:128] = real[:, 64:128]
        states[1, here, 0:64] = imag[:, 0:64]
        states[1, there, 64:128] = imag[:, 64:128]
    read_real, read_imag = halves_joined(read_mix_ref[0], read_mix_ref[1])
    read_out[...] = mm_across(states[0].astype(bf16), read_real.astype(bf16)) + mm_across(
        states[1].astype(bf16), read_imag.astype(bf16)
    )
    wide = iota((ROWS, 128), 1)
    mixed = skip_ref[...] * x_ref[...].astype(f32)
    for g in range(GROUPS):
        mixed = mixed + jnp.where(
            wide // 16 == g, read_out[pl.ds(g, ROWS, stride=GROUPS), :], 0.0
        )
    activated = jax.nn.gelu(mixed).astype(bf16)
    partial = mm(activated, out_weight_ref[...]).astype(bf16)
    for j in range(PEERS):
        partial_ref[j] = partial[:, 128 * j : 128 * (j + 1)]


def column(row):
    eye = iota((ROWS, ROWS), 0) == iota((ROWS, ROWS), 1)
    return jnp.sum(jnp.where(eye, row, 0.0), axis=1, keepdims=True)


def slots_down(routes, k):
    before = iota((ROWS, ROWS), 1) < iota((ROWS, ROWS), 0)
    expert = column(routes[k : k + 1])
    met = (expert == routes[0:1]).astype(f32) + (expert == routes[1:2]).astype(f32)
    rank = jnp.sum(jnp.where(before, met, 0.0), axis=1, keepdims=True)
    return expert * PAD + rank


def slots_across(routes, k):
    before = iota((ROWS, ROWS), 0) < iota((ROWS, ROWS), 1)
    expert = routes[k : k + 1]
    met = (column(routes[0:1]) == expert).astype(f32) + (column(routes[1:2]) == expert).astype(f32)
    rank = jnp.sum(jnp.where(before, met, 0.0), axis=0, keepdims=True)
    return expert * PAD + rank


def stream_body(arrived_ref, residual_ref, routes_ref, stream_ref, outgoing_ref):
    total = residual_ref[...].astype(f32)
    projected = arrived_ref[0].astype(f32)
    for j in range(1, PEERS):
        projected = projected + arrived_ref[j].astype(f32)
    stream = (total + projected).astype(bf16)
    stream_ref[...] = stream
    routes = routes_ref[...].astype(f32)
    slot = iota((BLOCKS * PAD, ROWS), 0).astype(f32)
    placing = (slot == slots_across(routes, 0)).astype(f32) + (
        slot == slots_across(routes, 1)
    ).astype(f32)
    outgoing_ref[...] = mm(placing.astype(bf16), stream).astype(bf16)


def packed_rows(shape, packed_dim):
    packed, padded = iota(shape, packed_dim), iota(shape, 1 - packed_dim)
    block = padded // PAD
    slot = padded - block * PAD
    return ((slot < SLOTS) & (packed == block * SLOTS + slot)).astype(f32).astype(bf16)


def copies_body(arrived_ref, gain_ref, copies_ref):
    rows = mm(packed_rows((EROWS, BLOCKS * PAD), 0), arrived_ref[...]).astype(bf16)
    gain = gain_ref[...]
    high = gain.astype(bf16).astype(f32)
    middle = (gain - high).astype(bf16).astype(f32)
    low = gain - high - middle
    row = iota((16, 128), 0)
    gains = jnp.where(
        row == 0, high, jnp.where(row == 1, middle, jnp.where(row == 2, low, 0.0))
    ).astype(bf16)
    for j in range(PEERS):
        copies_ref[j, 0:EROWS, :] = rows
        copies_ref[j, EROWS:SENT, :] = gains


def expert_body(rows_ref, gate_ref, up_ref, down_ref, terms_ref, normed):
    squares = jnp.zeros((EROWS, 128), f32)
    for j in range(PEERS):
        piece = rows_ref[j, 0:EROWS, :].astype(f32)
        squares = squares + piece * piece
    mean = jnp.sum(squares, axis=1, keepdims=True) / (128 * PEERS)
    factor = lax.rsqrt(mean + epsilon)
    for j in range(PEERS):
        gains = rows_ref[j, EROWS:SENT, :].astype(f32)
        gain = gains[0:1] + gains[1:2] + gains[2:3]
        piece = rows_ref[j, 0:EROWS, :].astype(f32)
        normed[:, 128 * j : 128 * (j + 1)] = (piece * factor * gain).astype(bf16)
    rows = normed[...]
    gate = mm(rows, gate_ref[0])
    up = mm(rows, up_ref[0])
    hidden = (jax.nn.silu(gate) * up).astype(bf16)
    terms = mm(hidden, down_ref[0]).astype(bf16)
    for j in range(PEERS):
        terms_ref[j] = terms[:, 128 * j : 128 * (j + 1)]


def answer_body(terms_ref, answer_ref):
    total = terms_ref[0].astype(f32)
    for j in range(1, PEERS):
        total = total + terms_ref[j].astype(f32)
    answer_ref[...] = mm(packed_rows((BLOCKS * PAD, EROWS), 1), total.astype(bf16)).astype(bf16)


def mixture_body(returned_ref, stream_ref, routes_ref, weight_ref, out_ref):
    routes, returned = routes_ref[...].astype(f32), returned_ref[...]
    slot = iota((ROWS, BLOCKS * PAD), 1).astype(f32)
    mixture = jnp.zeros((ROWS, 128), f32)
    for k in range(2):
        pick = (slot == slots_down(routes, k)).astype(f32).astype(bf16)
        mixture = mixture + mm(pick, returned) * column(weight_ref[k : k + 1, :])
    out_ref[...] = (stream_ref[...].astype(f32) + mixture).astype(bf16)


def exchanged(pieces, axis):
    return lax.all_to_all(pieces, axis, 0, 0, tiled=True)


def shards(
    mixer_in,
    residual,
    doc_ids,
    log_step,
    log_extra,
    in_mix,
    read_mix,
    skip_gain,
    out_weight,
    norm_gain,
    routes,
    route_weight,
    switch_matrices,
    up_weight,
    down_weight,
):
    me = lax.axis_index("sp").reshape(1)
    tall = GROUPS * ROWS
    message, real, imag, keep, turn = call(
        sweep_body,
        [SMEM, SMEM, VMEM, VMEM, VMEM, VMEM],
        [
            ((BLOCKS, 16, 128), bf16),
            ((ROWS, GROUPS, 128), f32),
            ((ROWS, GROUPS, 128), f32),
            ((ROWS, GROUPS, 128), f32),
            ((2, GROUPS, 128), f32),
        ],
        [((tall, 128), f32), ((2, tall, 128), f32), ((tall, 128), f32)],
    )(me, doc_ids, log_step, log_extra.T, mixer_in, in_mix.reshape(2, 128, 128))
    messages = near(exchanged(message, "sp"))
    (partial,) = call(
        mixer_body,
        [SMEM, SMEM] + [VMEM] * 9,
        [((PEERS, ROWS, 128), bf16)],
        [((2, tall, 128), f32), ((tall, 128), f32)],
    )(
        me, doc_ids, messages, near(real), near(imag), near(keep), near(turn), mixer_in,
        read_mix.swapaxes(2, 3).reshape(2, 128, 128), skip_gain.reshape(1, 128),
        out_weight,
    )
    shares = near(exchanged(partial, TP))
    stream, outgoing = call(
        stream_body,
        [VMEM] * 3,
        [((ROWS, 128), bf16), ((BLOCKS * PAD, 128), bf16)],
    )(shares, residual, routes.T)
    arrived = exchanged(outgoing.reshape(BLOCKS, PAD, 128), "sp").reshape(BLOCKS * PAD, 128)
    (copies,) = call(copies_body, [VMEM] * 2, [((PEERS, SENT, 128), bf16)])(
        near(arrived), norm_gain.reshape(1, 128)
    )
    (terms,) = call(
        expert_body,
        [VMEM] * 4,
        [((PEERS, EROWS, 128), bf16)],
        [((EROWS, 128 * PEERS), bf16)],
    )(near(exchanged(copies, TP)), switch_matrices, up_weight, down_weight)
    (answer,) = call(answer_body, [VMEM], [((BLOCKS * PAD, 128), bf16)])(
        near(exchanged(terms, TP))
    )
    returned = exchanged(answer.reshape(BLOCKS, PAD, 128), "sp").reshape(BLOCKS * PAD, 128)
    (out,) = call(mixture_body, [VMEM] * 4, [((ROWS, 128), bf16)], last=True)(
        near(returned), near(stream), routes.T, route_weight.T
    )
    return out


def solution(mesh):
    split = Mesh(mesh.devices.reshape(mesh.shape["sp"], 4, 4), ("sp", "tp_0", "tp_1"))
    in_specs = (
        P("sp", TP),
        P("sp", TP),
        P("sp"),
        P(None, TP),
        P("sp", TP),
        P(None, TP, None, None),
        P(None, TP, None, None),
        P(TP),
        P(TP, None),
        P(TP),
        P("sp", None),
        P("sp", None),
        P("sp", None, TP),
        P("sp", None, TP),
        P("sp", TP, None),
    )
    out_specs = P("sp", TP)
    return jax.shard_map(
        shards, mesh=split, in_specs=in_specs, out_specs=out_specs, check_vma=False
    )
```

```python
import jax
import jax.numpy as jnp
from jax import lax
from jax.experimental import pallas as pl
from jax.experimental.pallas import tpu as pltpu
from jax.sharding import Mesh
from jax.sharding import PartitionSpec as P

TP = ("tp_0", "tp_1")
INTERPRET = False

epsilon = 1e-06
f32 = jnp.float32
bf16 = jnp.bfloat16

BLOCKS = 32
PEERS = 16
ROWS = 64
GROUPS = 8
SLOTS = 5
PAD = 8
EROWS = BLOCKS * SLOTS
SENT = EROWS + 16

VMEM = pl.BlockSpec(memory_space=pltpu.VMEM)
SMEM = pl.BlockSpec(memory_space=pltpu.SMEM)
FAR = pl.BlockSpec(memory_space=pl.ANY if INTERPRET else pltpu.HBM)


def near(x):
    return x if INTERPRET else pltpu.with_memory_space_constraint(x, pltpu.VMEM)


def far(x):
    return x if INTERPRET else pltpu.with_memory_space_constraint(x, pltpu.HBM)


def call(body, in_specs, outs, scratch=(), copies=0, last=False):
    kept = jax.ShapeDtypeStruct if INTERPRET or last else pltpu.VMEM
    return pl.pallas_call(
        body,
        in_specs=in_specs,
        out_specs=[VMEM] * len(outs),
        out_shape=[kept(shape, dtype) for shape, dtype in outs],
        scratch_shapes=[
            (pltpu.SMEM if dtype == jnp.int32 else pltpu.VMEM)(shape, dtype)
            for shape, dtype in scratch
        ]
        + ([pltpu.SemaphoreType.DMA((copies,))] if copies else []),
        compiler_params=pltpu.CompilerParams(vmem_limit_bytes=16 * 2**20),
        interpret=INTERPRET,
    )


def iota(shape, dim):
    return lax.broadcasted_iota(jnp.int32, shape, dim)


def mm(a, b):
    return jnp.dot(a, b, preferred_element_type=f32)


def mm_across(a, b):
    return lax.dot_general(a, b, (((1,), (1,)), ((), ())), preferred_element_type=f32)


def halves_joined(first, second):
    left = iota((128, 128), 1) < 64
    return (
        jnp.where(left, first, pltpu.roll(second, 64, 1)),
        jnp.where(left, pltpu.roll(first, 64, 1), second),
    )


def steps_by_lane(log_step):
    eye = iota((GROUPS, GROUPS), 0) == iota((GROUPS, GROUPS), 1)
    step = jnp.exp(log_step)
    columns = [
        jnp.sum(
            jnp.where(eye, jnp.broadcast_to(step[k : k + 1, :], (GROUPS, GROUPS)), 0.0),
            axis=1,
            keepdims=True,
        )
        for k in range(2)
    ]
    return jnp.where(iota((GROUPS, 128), 1) < 64, columns[0], columns[1])


def one_minus_exp(x):
    series = jnp.ones_like(x)
    for n in range(9, 1, -1):
        series = 1.0 - x * (1.0 / n) * series
    return jnp.where(x < 0.5, x * series, 1.0 - jnp.exp(-x))


def sweep_body(
    me_ref, far_docs, far_step, far_extra, far_x, far_mix,
    message_ref, real_ref, imag_ref, keep_ref, turn_ref,
    masked, source, magnitude, log_step_ref, log_extra_ref, x_ref, in_mix_ref, docs_ref, arrivals,
):
    here_now = [
        pltpu.make_async_copy(far, near_ref, arrivals.at[k])
        for k, (far, near_ref) in enumerate(
            [
                (far_mix, in_mix_ref),
                (far_x, x_ref),
                (far_extra, log_extra_ref),
                (far_step, log_step_ref),
                (far_docs, docs_ref),
            ]
        )
    ]
    for copy in here_now:
        copy.start()
    for copy in here_now[::-1]:
        copy.wait()
    lane = iota((GROUPS, 128), 1)
    fwd = lane < 64
    step = steps_by_lane(log_step_ref[...])
    theta = (jnp.pi * (lane & 63).astype(f32)) * step
    cos, sin = jnp.cos(theta), jnp.sin(theta)
    turn_ref[0] = cos
    turn_ref[1] = sin
    scale = jnp.sqrt(one_minus_exp(step))
    wide = iota((ROWS, 128), 1)
    x = x_ref[...].astype(f32)
    for g in range(GROUPS):
        masked[pl.ds(g, ROWS, stride=GROUPS), :] = jnp.where(wide // 16 == g, x, 0.0)
    log_extra = log_extra_ref[...]
    loss = -0.5 * step
    for n in range(ROWS):
        extra = jnp.broadcast_to(log_extra[:, n : n + 1], (GROUPS, 128))
        magnitude[pl.ds(GROUPS * n, GROUPS), :] = jnp.exp(loss + extra)
    mix_real, mix_imag = halves_joined(in_mix_ref[0], in_mix_ref[1])
    rows = masked[...].astype(bf16)
    source[0] = mm(rows, mix_real.astype(bf16))
    source[1] = mm(rows, mix_imag.astype(bf16))
    real = jnp.zeros((GROUPS, 128), f32)
    imag = jnp.zeros((GROUPS, 128), f32)
    total = jnp.ones((GROUPS, 128), f32)
    for n in range(ROWS):
        r = ROWS - 1 - n
        here, there = pl.ds(GROUPS * n, GROUPS), pl.ds(GROUPS * r, GROUPS)
        keep = jnp.where(fwd, magnitude[here, :], magnitude[there, :])
        if n > 0:
            same_fwd = jnp.where(docs_ref[n] == docs_ref[n - 1], 1.0, 0.0)
            same_bwd = jnp.where(docs_ref[r] == docs_ref[r + 1], 1.0, 0.0)
            keep = keep * jnp.where(fwd, same_fwd, same_bwd)
        new_real = scale * jnp.where(fwd, source[0, here, :], source[0, there, :])
        new_imag = scale * jnp.where(fwd, source[1, here, :], source[1, there, :])
        keep_ref[n] = keep
        real_ref[n] = new_real
        imag_ref[n] = new_imag
        by_cos, by_sin = keep * cos, keep * sin
        real, imag = (
            (by_cos * real + new_real) - by_sin * imag,
            (by_sin * real + new_imag) + by_cos * imag,
        )
        total = total * keep
    crossed = pltpu.roll(total, 64, 1)
    high = crossed.astype(bf16).astype(f32)
    decay = jnp.where((lane & 32) == 0, high, crossed - high)
    first_doc = docs_ref[0].astype(f32)
    last_doc = docs_ref[ROWS - 1].astype(f32)
    turn_ref[2] = jnp.where(fwd, first_doc, last_doc)
    to_later = jnp.concatenate(
        [jnp.where(fwd, real, decay), jnp.where(fwd, imag, last_doc)], axis=0
    ).astype(bf16)
    to_earlier = jnp.concatenate(
        [jnp.where(fwd, decay, real), jnp.where(fwd, first_doc, imag)], axis=0
    ).astype(bf16)
    me = me_ref[0]
    for i in range(BLOCKS):
        @pl.when(me < i)
        def _():
            message_ref[i] = to_later

        @pl.when(me >= i)
        def _():
            message_ref[i] = to_earlier


def mixer_body(
    me_ref, message_ref, real_ref, imag_ref, keep_ref, turn_ref,
    far_x, far_read, far_skip, far_weight,
    partial_ref,
    states, read_out, x_ref, read_mix_ref, skip_ref, out_weight_ref, arrivals,
):
    here_now = [
        pltpu.make_async_copy(far, near_ref, arrivals.at[k])
        for k, (far, near_ref) in enumerate(
            [(far_read, read_mix_ref), (far_x, x_ref), (far_skip, skip_ref), (far_weight, out_weight_ref)]
        )
    ]
    for copy in here_now:
        copy.start()
    lane = iota((GROUPS, 128), 1)
    fwd = lane < 64
    odd = (lane & 32) != 0
    me = me_ref[0]
    cos, sin, mine = turn_ref[0], turn_ref[1], turn_ref[2]
    block_cos, block_sin = cos, sin
    for _ in range(6):
        block_cos, block_sin = (
            block_cos * block_cos - block_sin * block_sin,
            2.0 * block_cos * block_sin,
        )
    real = jnp.zeros((GROUPS, 128), f32)
    imag = jnp.zeros((GROUPS, 128), f32)
    for n in range(BLOCKS - 1):
        r = BLOCKS - 1 - n
        one, two = message_ref[n].astype(f32), message_ref[r].astype(f32)
        decay = pltpu.roll(jnp.where(fwd, two[:GROUPS], one[:GROUPS]), 64, 1)
        decay = decay + jnp.where(odd, pltpu.roll(decay, 32, 1), pltpu.roll(decay, 96, 1))
        doc = pltpu.roll(jnp.where(fwd, two[GROUPS:], one[GROUPS:]), 64, 1)
        same = doc == mine
        new_real = jnp.where(same, jnp.where(fwd, one[:GROUPS], two[:GROUPS]), 0.0)
        new_imag = jnp.where(same, jnp.where(fwd, one[GROUPS:], two[GROUPS:]), 0.0)
        by_cos, by_sin = decay * block_cos, decay * block_sin
        passed = jnp.where(fwd, (n < me).astype(jnp.int32), (r > me).astype(jnp.int32)) > 0
        real, imag = (
            jnp.where(passed, (by_cos * real + new_real) - by_sin * imag, real),
            jnp.where(passed, (by_sin * real + new_imag) + by_cos * imag, imag),
        )
    for n in range(ROWS):
        r = ROWS - 1 - n
        here, there = pl.ds(GROUPS * n, GROUPS), pl.ds(GROUPS * r, GROUPS)
        keep = keep_ref[n]
        by_cos, by_sin = keep * cos, keep * sin
        real, imag = (
            (by_cos * real + real_ref[n]) - by_sin * imag,
            (by_sin * real + imag_ref[n]) + by_cos * imag,
        )
        states[0, here, 0:64] = real[:, 0:64]
        states[0, there, 64:128] = real[:, 64:128]
        states[1, here, 0:64] = imag[:, 0:64]
        states[1, there, 64:128] = imag[:, 64:128]
    for copy in here_now:
        copy.wait()
    read_real, read_imag = halves_joined(read_mix_ref[0], read_mix_ref[1])
    read_out[...] = mm_across(states[0].astype(bf16), read_real.astype(bf16)) + mm_across(
        states[1].astype(bf16), read_imag.astype(bf16)
    )
    wide = iota((ROWS, 128), 1)
    mixed = skip_ref[...] * x_ref[...].astype(f32)
    for g in range(GROUPS):
        mixed = mixed + jnp.where(
            wide // 16 == g, read_out[pl.ds(g, ROWS, stride=GROUPS), :], 0.0
        )
    activated = jax.nn.gelu(mixed).astype(bf16)
    partial = mm(activated, out_weight_ref[...]).astype(bf16)
    for j in range(PEERS):
        partial_ref[j] = partial[:, 128 * j : 128 * (j + 1)]


def column(row):
    eye = iota((ROWS, ROWS), 0) == iota((ROWS, ROWS), 1)
    return jnp.sum(jnp.where(eye, row, 0.0), axis=1, keepdims=True)


def slots_down(routes, k):
    before = iota((ROWS, ROWS), 1) < iota((ROWS, ROWS), 0)
    expert = column(routes[k : k + 1])
    met = (expert == routes[0:1]).astype(f32) + (expert == routes[1:2]).astype(f32)
    rank = jnp.sum(jnp.where(before, met, 0.0), axis=1, keepdims=True)
    return expert * PAD + rank


def slots_across(routes, k):
    before = iota((ROWS, ROWS), 0) < iota((ROWS, ROWS), 1)
    expert = routes[k : k + 1]
    met = (column(routes[0:1]) == expert).astype(f32) + (column(routes[1:2]) == expert).astype(f32)
    rank = jnp.sum(jnp.where(before, met, 0.0), axis=0, keepdims=True)
    return expert * PAD + rank


def stream_body(
    arrived_ref, residual_ref, routes_ref, weight_ref, stream_ref, outgoing_ref, weights_ref
):
    weights_ref[...] = weight_ref[...]
    total = residual_ref[...].astype(f32)
    projected = arrived_ref[0].astype(f32)
    for j in range(1, PEERS):
        projected = projected + arrived_ref[j].astype(f32)
    stream = (total + projected).astype(bf16)
    stream_ref[...] = stream
    routes = routes_ref[...].astype(f32)
    slot = iota((BLOCKS * PAD, ROWS), 0).astype(f32)
    placing = (slot == slots_across(routes, 0)).astype(f32) + (
        slot == slots_across(routes, 1)
    ).astype(f32)
    outgoing_ref[...] = mm(placing.astype(bf16), stream).astype(bf16)


def packed_rows(shape, packed_dim):
    packed, padded = iota(shape, packed_dim), iota(shape, 1 - packed_dim)
    block = padded // PAD
    slot = padded - block * PAD
    return ((slot < SLOTS) & (packed == block * SLOTS + slot)).astype(f32).astype(bf16)


def copies_body(arrived_ref, gain_ref, copies_ref):
    rows = mm(packed_rows((EROWS, BLOCKS * PAD), 0), arrived_ref[...]).astype(bf16)
    gain = gain_ref[...]
    high = gain.astype(bf16).astype(f32)
    middle = (gain - high).astype(bf16).astype(f32)
    low = gain - high - middle
    row = iota((16, 128), 0)
    gains = jnp.where(
        row == 0, high, jnp.where(row == 1, middle, jnp.where(row == 2, low, 0.0))
    ).astype(bf16)
    for j in range(PEERS):
        copies_ref[j, 0:EROWS, :] = rows
        copies_ref[j, EROWS:SENT, :] = gains


def expert_body(rows_ref, gate_ref, up_ref, down_ref, terms_ref, normed):
    squares = jnp.zeros((EROWS, 128), f32)
    for j in range(PEERS):
        piece = rows_ref[j, 0:EROWS, :].astype(f32)
        squares = squares + piece * piece
    mean = jnp.sum(squares, axis=1, keepdims=True) / (128 * PEERS)
    factor = lax.rsqrt(mean + epsilon)
    for j in range(PEERS):
        gains = rows_ref[j, EROWS:SENT, :].astype(f32)
        gain = gains[0:1] + gains[1:2] + gains[2:3]
        piece = rows_ref[j, 0:EROWS, :].astype(f32)
        normed[:, 128 * j : 128 * (j + 1)] = (piece * factor * gain).astype(bf16)
    rows = normed[...]
    gate = mm(rows, gate_ref[0])
    up = mm(rows, up_ref[0])
    hidden = (jax.nn.silu(gate) * up).astype(bf16)
    terms = mm(hidden, down_ref[0]).astype(bf16)
    for j in range(PEERS):
        terms_ref[j] = terms[:, 128 * j : 128 * (j + 1)]


def answer_body(terms_ref, answer_ref):
    total = terms_ref[0].astype(f32)
    for j in range(1, PEERS):
        total = total + terms_ref[j].astype(f32)
    answer_ref[...] = mm(packed_rows((BLOCKS * PAD, EROWS), 1), total.astype(bf16)).astype(bf16)


def mixture_body(returned_ref, stream_ref, routes_ref, weight_ref, out_ref):
    routes, returned = routes_ref[...].astype(f32), returned_ref[...]
    slot = iota((ROWS, BLOCKS * PAD), 1).astype(f32)
    mixture = jnp.zeros((ROWS, 128), f32)
    for k in range(2):
        pick = (slot == slots_down(routes, k)).astype(f32).astype(bf16)
        mixture = mixture + mm(pick, returned) * column(weight_ref[k : k + 1, :])
    out_ref[...] = (stream_ref[...].astype(f32) + mixture).astype(bf16)


def exchanged(pieces, axis):
    return lax.all_to_all(pieces, axis, 0, 0, tiled=True)


def shards(
    mixer_in,
    residual,
    doc_ids,
    log_step,
    log_extra,
    in_mix,
    read_mix,
    skip_gain,
    out_weight,
    norm_gain,
    routes,
    route_weight,
    switch_matrices,
    up_weight,
    down_weight,
):
    me = lax.axis_index("sp").reshape(1)
    tall = GROUPS * ROWS
    message, real, imag, keep, turn = call(
        sweep_body,
        [SMEM, FAR, FAR, FAR, FAR, FAR],
        [
            ((BLOCKS, 16, 128), bf16),
            ((ROWS, GROUPS, 128), f32),
            ((ROWS, GROUPS, 128), f32),
            ((ROWS, GROUPS, 128), f32),
            ((3, GROUPS, 128), f32),
        ],
        [
            ((tall, 128), f32),
            ((2, tall, 128), f32),
            ((tall, 128), f32),
            ((2, GROUPS), f32),
            ((GROUPS, ROWS), f32),
            ((ROWS, 128), bf16),
            ((2, 128, 128), f32),
            ((ROWS,), jnp.int32),
        ],
        copies=5,
    )(
        me, far(doc_ids), far(log_step), far(log_extra.T), far(mixer_in), far(in_mix.reshape(2, 128, 128))
    )
    messages = near(exchanged(message, "sp"))
    (partial,) = call(
        mixer_body,
        [SMEM] + [VMEM] * 5 + [FAR] * 4,
        [((PEERS, ROWS, 128), bf16)],
        [
            ((2, tall, 128), f32),
            ((tall, 128), f32),
            ((ROWS, 128), bf16),
            ((2, 128, 128), f32),
            ((1, 128), f32),
            ((128, 128 * PEERS), bf16),
        ],
        copies=4,
    )(
        me, messages, near(real), near(imag), near(keep), near(turn), far(mixer_in),
        far(read_mix.swapaxes(2, 3).reshape(2, 128, 128)), far(skip_gain.reshape(1, 128)),
        far(out_weight),
    )
    shares = near(exchanged(partial, TP))
    stream, outgoing, weights = call(
        stream_body,
        [VMEM] * 4,
        [((ROWS, 128), bf16), ((BLOCKS * PAD, 128), bf16), ((2, ROWS), f32)],
    )(shares, residual, routes.T, route_weight.T)
    arrived = exchanged(outgoing.reshape(BLOCKS, PAD, 128), "sp").reshape(BLOCKS * PAD, 128)
    (copies,) = call(copies_body, [VMEM] * 2, [((PEERS, SENT, 128), bf16)])(
        near(arrived), norm_gain.reshape(1, 128)
    )
    (terms,) = call(
        expert_body,
        [VMEM] * 4,
        [((PEERS, EROWS, 128), bf16)],
        [((EROWS, 128 * PEERS), bf16)],
    )(near(exchanged(copies, TP)), switch_matrices, up_weight, down_weight)
    (answer,) = call(answer_body, [VMEM], [((BLOCKS * PAD, 128), bf16)])(
        near(exchanged(terms, TP))
    )
    returned = exchanged(answer.reshape(BLOCKS, PAD, 128), "sp").reshape(BLOCKS * PAD, 128)
    (out,) = call(mixture_body, [VMEM] * 4, [((ROWS, 128), bf16)], last=True)(
        near(returned), near(stream), routes.T, near(weights)
    )
    return out


def solution(mesh):
    split = Mesh(mesh.devices.reshape(mesh.shape["sp"], 4, 4), ("sp", "tp_0", "tp_1"))
    in_specs = (
        P("sp", TP),
        P("sp", TP),
        P("sp"),
        P(None, TP),
        P("sp", TP),
        P(None, TP, None, None),
        P(None, TP, None, None),
        P(TP),
        P(TP, None),
        P(TP),
        P("sp", None),
        P("sp", None),
        P("sp", None, TP),
        P("sp", None, TP),
        P("sp", TP, None),
    )
    out_specs = P("sp", TP)
    return jax.shard_map(
        shards, mesh=split, in_specs=in_specs, out_specs=out_specs, check_vma=False
    )
```

```python
import jax
import jax.numpy as jnp
from jax import lax
from jax.experimental import pallas as pl
from jax.experimental.pallas import tpu as pltpu
from jax.sharding import Mesh
from jax.sharding import PartitionSpec as P

TP = ("tp_0", "tp_1")
INTERPRET = False

epsilon = 1e-06
f32 = jnp.float32
bf16 = jnp.bfloat16

BLOCKS = 32
PEERS = 16
ROWS = 64
GROUPS = 8
SLOTS = 5
PAD = 6
LINES = 10
EROWS = BLOCKS * SLOTS
SENT = EROWS + 16

VMEM = pl.BlockSpec(memory_space=pltpu.VMEM)
SMEM = pl.BlockSpec(memory_space=pltpu.SMEM)
FAR = pl.BlockSpec(memory_space=pl.ANY if INTERPRET else pltpu.HBM)


def near(x):
    return x if INTERPRET else pltpu.with_memory_space_constraint(x, pltpu.VMEM)


def far(x):
    return x if INTERPRET else pltpu.with_memory_space_constraint(x, pltpu.HBM)


def call(body, in_specs, outs, scratch=(), copies=0, last=False):
    kept = jax.ShapeDtypeStruct if INTERPRET or last else pltpu.VMEM
    return pl.pallas_call(
        body,
        in_specs=in_specs,
        out_specs=[VMEM] * len(outs),
        out_shape=[kept(shape, dtype) for shape, dtype in outs],
        scratch_shapes=[
            (pltpu.SMEM if dtype == jnp.int32 else pltpu.VMEM)(shape, dtype)
            for shape, dtype in scratch
        ]
        + ([pltpu.SemaphoreType.DMA((copies,))] if copies else []),
        compiler_params=pltpu.CompilerParams(vmem_limit_bytes=16 * 2**20),
        interpret=INTERPRET,
    )


def iota(shape, dim):
    return lax.broadcasted_iota(jnp.int32, shape, dim)


def divided(x, by):
    return (x * (65536 // by + 1)) >> 16


def mm(a, b):
    return jnp.dot(a, b, preferred_element_type=f32)


def mm_across(a, b):
    return lax.dot_general(a, b, (((1,), (1,)), ((), ())), preferred_element_type=f32)


def halves_joined(first, second):
    left = iota((128, 128), 1) < 64
    return (
        jnp.where(left, first, pltpu.roll(second, 64, 1)),
        jnp.where(left, pltpu.roll(first, 64, 1), second),
    )


def steps_by_lane(log_step):
    eye = iota((GROUPS, GROUPS), 0) == iota((GROUPS, GROUPS), 1)
    step = jnp.exp(log_step)
    columns = [
        jnp.sum(
            jnp.where(eye, jnp.broadcast_to(step[k : k + 1, :], (GROUPS, GROUPS)), 0.0),
            axis=1,
            keepdims=True,
        )
        for k in range(2)
    ]
    return jnp.where(iota((GROUPS, 128), 1) < 64, columns[0], columns[1])


def one_minus_exp(x):
    series = jnp.ones_like(x)
    for n in range(9, 1, -1):
        series = 1.0 - x * (1.0 / n) * series
    return jnp.where(x < 0.5, x * series, 1.0 - jnp.exp(-x))


def sweep_body(
    me_ref, far_docs, far_step, far_extra, far_x, far_mix,
    message_ref, real_ref, imag_ref, keep_ref, turn_ref,
    masked, source, magnitude, log_step_ref, log_extra_ref, x_ref, in_mix_ref, docs_ref, arrivals,
):
    here_now = [
        pltpu.make_async_copy(far, near_ref, arrivals.at[k])
        for k, (far, near_ref) in enumerate(
            [
                (far_mix, in_mix_ref),
                (far_x, x_ref),
                (far_extra, log_extra_ref),
                (far_step, log_step_ref),
                (far_docs, docs_ref),
            ]
        )
    ]
    for copy in here_now:
        copy.start()
    for copy in here_now[::-1]:
        copy.wait()
    lane = iota((GROUPS, 128), 1)
    fwd = lane < 64
    step = steps_by_lane(log_step_ref[...])
    theta = (jnp.pi * (lane & 63).astype(f32)) * step
    cos, sin = jnp.cos(theta), jnp.sin(theta)
    turn_ref[0] = cos
    turn_ref[1] = sin
    scale = jnp.sqrt(one_minus_exp(step))
    wide = iota((ROWS, 128), 1)
    x = x_ref[...].astype(f32)
    for g in range(GROUPS):
        masked[pl.ds(g, ROWS, stride=GROUPS), :] = jnp.where(wide // 16 == g, x, 0.0)
    log_extra = log_extra_ref[...]
    loss = -0.5 * step
    for n in range(ROWS):
        extra = jnp.broadcast_to(log_extra[:, n : n + 1], (GROUPS, 128))
        magnitude[pl.ds(GROUPS * n, GROUPS), :] = jnp.exp(loss + extra)
    mix_real, mix_imag = halves_joined(in_mix_ref[0], in_mix_ref[1])
    rows = masked[...].astype(bf16)
    source[0] = mm(rows, mix_real.astype(bf16))
    source[1] = mm(rows, mix_imag.astype(bf16))
    real = jnp.zeros((GROUPS, 128), f32)
    imag = jnp.zeros((GROUPS, 128), f32)
    total = jnp.ones((GROUPS, 128), f32)
    for n in range(ROWS):
        r = ROWS - 1 - n
        here, there = pl.ds(GROUPS * n, GROUPS), pl.ds(GROUPS * r, GROUPS)
        keep = jnp.where(fwd, magnitude[here, :], magnitude[there, :])
        if n > 0:
            same_fwd = jnp.where(docs_ref[n] == docs_ref[n - 1], 1.0, 0.0)
            same_bwd = jnp.where(docs_ref[r] == docs_ref[r + 1], 1.0, 0.0)
            keep = keep * jnp.where(fwd, same_fwd, same_bwd)
        new_real = scale * jnp.where(fwd, source[0, here, :], source[0, there, :])
        new_imag = scale * jnp.where(fwd, source[1, here, :], source[1, there, :])
        keep_ref[n] = keep
        real_ref[n] = new_real
        imag_ref[n] = new_imag
        by_cos, by_sin = keep * cos, keep * sin
        real, imag = (
            (by_cos * real + new_real) - by_sin * imag,
            (by_sin * real + new_imag) + by_cos * imag,
        )
        total = total * keep
    high = total.astype(bf16).astype(f32)
    low = total - high
    first_doc = docs_ref[0].astype(f32)
    last_doc = docs_ref[ROWS - 1].astype(f32)
    turn_ref[2] = jnp.where(fwd, first_doc, last_doc)
    group = iota((GROUPS, 128), 0)
    lines = []
    for kept, doc, left, right in [
        (0, last_doc, real, pltpu.roll(imag, 64, 1)),
        (64, first_doc, pltpu.roll(imag, 64, 1), real),
    ]:
        decays = jnp.where(lane == kept + group, high, 0.0) + jnp.where(
            lane == kept + GROUPS + group, low, 0.0
        )
        row = jnp.sum(decays, axis=0, keepdims=True) + jnp.where(
            lane[0:1] == kept + 2 * GROUPS, doc, 0.0
        )
        lines.append(jnp.where(fwd, left, right))
        lines.append(jnp.broadcast_to(row, (GROUPS, 128)))
    lines = jnp.concatenate(lines, axis=0).astype(bf16)
    row, entry = iota((BLOCKS * LINES, 32), 0), iota((BLOCKS * LINES, 32), 1)
    receiver = divided(row, LINES)
    wanted = row - receiver * LINES + jnp.where(receiver > me_ref[0], 0, 16)
    message_ref[...] = mm((entry == wanted).astype(f32).astype(bf16), lines).astype(bf16)


def mixer_body(
    me_ref, messages_ref, real_ref, imag_ref, keep_ref, turn_ref,
    far_x, far_read, far_skip, far_weight,
    partial_ref,
    states, read_out, received, x_ref, read_mix_ref, skip_ref, out_weight_ref, arrivals,
):
    here_now = [
        pltpu.make_async_copy(far, near_ref, arrivals.at[k])
        for k, (far, near_ref) in enumerate(
            [(far_read, read_mix_ref), (far_x, x_ref), (far_skip, skip_ref), (far_weight, out_weight_ref)]
        )
    ]
    for copy in here_now:
        copy.start()
    lane = iota((GROUPS, 128), 1)
    fwd = lane < 64
    me = me_ref[0]
    cos, sin, mine = turn_ref[0], turn_ref[1], turn_ref[2]
    block_cos, block_sin = cos, sin
    for _ in range(6):
        block_cos, block_sin = (
            block_cos * block_cos - block_sin * block_sin,
            2.0 * block_cos * block_sin,
        )
    row, entry = iota((BLOCKS * 16, BLOCKS * LINES), 0), iota((BLOCKS * 16, BLOCKS * LINES), 1)
    wanted = (row >> 4) * LINES + jnp.minimum(row & 15, LINES - 1)
    received[...] = mm((entry == wanted).astype(f32).astype(bf16), messages_ref[...])
    group = iota((GROUPS, 128), 0)
    decays, docs = [], []
    for n in range(BLOCKS):
        kept = received[16 * n + GROUPS : 16 * (n + 1), :]
        place = lane & 63
        of_group = (place == group) | (place == GROUPS + group)
        decays.append(jnp.sum(jnp.where(of_group, kept, 0.0), axis=1, keepdims=True))
        docs.append(jnp.sum(jnp.where(place == 2 * GROUPS, kept, 0.0), axis=1, keepdims=True))
    real = jnp.zeros((GROUPS, 128), f32)
    imag = jnp.zeros((GROUPS, 128), f32)
    for n in range(BLOCKS - 1):
        r = BLOCKS - 1 - n
        one = received[16 * n : 16 * n + GROUPS, :]
        two = received[16 * r : 16 * r + GROUPS, :]
        decay = jnp.where(fwd, decays[n], decays[r])
        same = jnp.where(fwd, docs[n], docs[r]) == mine
        new_real = jnp.where(same, jnp.where(fwd, one, two), 0.0)
        new_imag = jnp.where(same, pltpu.roll(jnp.where(fwd, two, one), 64, 1), 0.0)
        by_cos, by_sin = decay * block_cos, decay * block_sin
        passed = jnp.where(fwd, (n < me).astype(jnp.int32), (r > me).astype(jnp.int32)) > 0
        real, imag = (
            jnp.where(passed, (by_cos * real + new_real) - by_sin * imag, real),
            jnp.where(passed, (by_sin * real + new_imag) + by_cos * imag, imag),
        )
    for n in range(ROWS):
        r = ROWS - 1 - n
        here, there = pl.ds(GROUPS * n, GROUPS), pl.ds(GROUPS * r, GROUPS)
        keep = keep_ref[n]
        by_cos, by_sin = keep * cos, keep * sin
        real, imag = (
            (by_cos * real + real_ref[n]) - by_sin * imag,
            (by_sin * real + imag_ref[n]) + by_cos * imag,
        )
        states[0, here, 0:64] = real[:, 0:64]
        states[0, there, 64:128] = real[:, 64:128]
        states[1, here, 0:64] = imag[:, 0:64]
        states[1, there, 64:128] = imag[:, 64:128]
    for copy in here_now:
        copy.wait()
    read_real, read_imag = halves_joined(read_mix_ref[0], read_mix_ref[1])
    read_out[...] = mm_across(states[0].astype(bf16), read_real.astype(bf16)) + mm_across(
        states[1].astype(bf16), read_imag.astype(bf16)
    )
    wide = iota((ROWS, 128), 1)
    mixed = skip_ref[...] * x_ref[...].astype(f32)
    for g in range(GROUPS):
        mixed = mixed + jnp.where(
            wide // 16 == g, read_out[pl.ds(g, ROWS, stride=GROUPS), :], 0.0
        )
    activated = jax.nn.gelu(mixed).astype(bf16)
    partial = mm(activated, out_weight_ref[...]).astype(bf16)
    for j in range(PEERS):
        partial_ref[j] = partial[:, 128 * j : 128 * (j + 1)]


def column(row):
    eye = iota((ROWS, ROWS), 0) == iota((ROWS, ROWS), 1)
    return jnp.sum(jnp.where(eye, row, 0.0), axis=1, keepdims=True)


def slots_down(routes, k):
    before = iota((ROWS, ROWS), 1) < iota((ROWS, ROWS), 0)
    expert = column(routes[k : k + 1])
    met = (expert == routes[0:1]).astype(f32) + (expert == routes[1:2]).astype(f32)
    rank = jnp.sum(jnp.where(before, met, 0.0), axis=1, keepdims=True)
    return expert * PAD + rank


def slots_across(routes, k):
    before = iota((ROWS, ROWS), 0) < iota((ROWS, ROWS), 1)
    expert = routes[k : k + 1]
    met = (column(routes[0:1]) == expert).astype(f32) + (column(routes[1:2]) == expert).astype(f32)
    rank = jnp.sum(jnp.where(before, met, 0.0), axis=0, keepdims=True)
    return expert * PAD + rank


def stream_body(
    arrived_ref, residual_ref, routes_ref, weight_ref, stream_ref, outgoing_ref, weights_ref
):
    weights_ref[...] = weight_ref[...]
    total = residual_ref[...].astype(f32)
    projected = arrived_ref[0].astype(f32)
    for j in range(1, PEERS):
        projected = projected + arrived_ref[j].astype(f32)
    stream = (total + projected).astype(bf16)
    stream_ref[...] = stream
    routes = routes_ref[...].astype(f32)
    slot = iota((BLOCKS * PAD, ROWS), 0).astype(f32)
    placing = (slot == slots_across(routes, 0)).astype(f32) + (
        slot == slots_across(routes, 1)
    ).astype(f32)
    outgoing_ref[...] = mm(placing.astype(bf16), stream).astype(bf16)


def packed_rows(shape, packed_dim):
    packed, padded = iota(shape, packed_dim), iota(shape, 1 - packed_dim)
    block = divided(padded, PAD)
    slot = padded - block * PAD
    return ((slot < SLOTS) & (packed == block * SLOTS + slot)).astype(f32).astype(bf16)


def copies_body(arrived_ref, gain_ref, copies_ref):
    rows = mm(packed_rows((EROWS, BLOCKS * PAD), 0), arrived_ref[...]).astype(bf16)
    gain = gain_ref[...]
    high = gain.astype(bf16).astype(f32)
    middle = (gain - high).astype(bf16).astype(f32)
    low = gain - high - middle
    row = iota((16, 128), 0)
    gains = jnp.where(
        row == 0, high, jnp.where(row == 1, middle, jnp.where(row == 2, low, 0.0))
    ).astype(bf16)
    for j in range(PEERS):
        copies_ref[j, 0:EROWS, :] = rows
        copies_ref[j, EROWS:SENT, :] = gains


def expert_body(rows_ref, gate_ref, up_ref, down_ref, terms_ref, normed):
    squares = jnp.zeros((EROWS, 128), f32)
    for j in range(PEERS):
        piece = rows_ref[j, 0:EROWS, :].astype(f32)
        squares = squares + piece * piece
    mean = jnp.sum(squares, axis=1, keepdims=True) / (128 * PEERS)
    factor = lax.rsqrt(mean + epsilon)
    for j in range(PEERS):
        gains = rows_ref[j, EROWS:SENT, :].astype(f32)
        gain = gains[0:1] + gains[1:2] + gains[2:3]
        piece = rows_ref[j, 0:EROWS, :].astype(f32)
        normed[:, 128 * j : 128 * (j + 1)] = (piece * factor * gain).astype(bf16)
    rows = normed[...]
    gate = mm(rows, gate_ref[0])
    up = mm(rows, up_ref[0])
    hidden = (jax.nn.silu(gate) * up).astype(bf16)
    terms = mm(hidden, down_ref[0]).astype(bf16)
    for j in range(PEERS):
        terms_ref[j] = terms[:, 128 * j : 128 * (j + 1)]


def answer_body(terms_ref, answer_ref):
    total = terms_ref[0].astype(f32)
    for j in range(1, PEERS):
        total = total + terms_ref[j].astype(f32)
    answer_ref[...] = mm(packed_rows((BLOCKS * PAD, EROWS), 1), total.astype(bf16)).astype(bf16)


def mixture_body(returned_ref, stream_ref, routes_ref, weight_ref, out_ref):
    routes, returned = routes_ref[...].astype(f32), returned_ref[...]
    slot = iota((ROWS, BLOCKS * PAD), 1).astype(f32)
    mixture = jnp.zeros((ROWS, 128), f32)
    for k in range(2):
        pick = (slot == slots_down(routes, k)).astype(f32).astype(bf16)
        mixture = mixture + mm(pick, returned) * column(weight_ref[k : k + 1, :])
    out_ref[...] = (stream_ref[...].astype(f32) + mixture).astype(bf16)


def exchanged(pieces, axis):
    return lax.all_to_all(pieces, axis, 0, 0, tiled=True)


def rows_exchanged(rows):
    pairs = rows.reshape(BLOCKS, rows.shape[0] // (2 * BLOCKS), 2, rows.shape[1])
    return exchanged(pairs, "sp").reshape(rows.shape)


def shards(
    mixer_in,
    residual,
    doc_ids,
    log_step,
    log_extra,
    in_mix,
    read_mix,
    skip_gain,
    out_weight,
    norm_gain,
    routes,
    route_weight,
    switch_matrices,
    up_weight,
    down_weight,
):
    me = lax.axis_index("sp").reshape(1)
    tall = GROUPS * ROWS
    message, real, imag, keep, turn = call(
        sweep_body,
        [SMEM, FAR, FAR, FAR, FAR, FAR],
        [
            ((BLOCKS * LINES, 128), bf16),
            ((ROWS, GROUPS, 128), f32),
            ((ROWS, GROUPS, 128), f32),
            ((ROWS, GROUPS, 128), f32),
            ((3, GROUPS, 128), f32),
        ],
        [
            ((tall, 128), f32),
            ((2, tall, 128), f32),
            ((tall, 128), f32),
            ((2, GROUPS), f32),
            ((GROUPS, ROWS), f32),
            ((ROWS, 128), bf16),
            ((2, 128, 128), f32),
            ((ROWS,), jnp.int32),
        ],
        copies=5,
    )(
        me, far(doc_ids), far(log_step), far(log_extra.T), far(mixer_in), far(in_mix.reshape(2, 128, 128))
    )
    messages = near(rows_exchanged(message))
    (partial,) = call(
        mixer_body,
        [SMEM] + [VMEM] * 5 + [FAR] * 4,
        [((PEERS, ROWS, 128), bf16)],
        [
            ((2, tall, 128), f32),
            ((tall, 128), f32),
            ((BLOCKS * 16, 128), f32),
            ((ROWS, 128), bf16),
            ((2, 128, 128), f32),
            ((1, 128), f32),
            ((128, 128 * PEERS), bf16),
        ],
        copies=4,
    )(
        me, messages, near(real), near(imag), near(keep), near(turn), far(mixer_in),
        far(read_mix.swapaxes(2, 3).reshape(2, 128, 128)), far(skip_gain.reshape(1, 128)),
        far(out_weight),
    )
    shares = near(exchanged(partial, TP))
    stream, outgoing, weights = call(
        stream_body,
        [VMEM] * 4,
        [((ROWS, 128), bf16), ((BLOCKS * PAD, 128), bf16), ((2, ROWS), f32)],
    )(shares, residual, routes.T, route_weight.T)
    arrived = rows_exchanged(outgoing)
    (copies,) = call(copies_body, [VMEM] * 2, [((PEERS, SENT, 128), bf16)])(
        near(arrived), norm_gain.reshape(1, 128)
    )
    (terms,) = call(
        expert_body,
        [VMEM] * 4,
        [((PEERS, EROWS, 128), bf16)],
        [((EROWS, 128 * PEERS), bf16)],
    )(near(exchanged(copies, TP)), switch_matrices, up_weight, down_weight)
    (answer,) = call(answer_body, [VMEM], [((BLOCKS * PAD, 128), bf16)])(
        near(exchanged(terms, TP))
    )
    returned = rows_exchanged(answer)
    (out,) = call(mixture_body, [VMEM] * 4, [((ROWS, 128), bf16)], last=True)(
        near(returned), near(stream), routes.T, near(weights)
    )
    return out


def solution(mesh):
    split = Mesh(mesh.devices.reshape(mesh.shape["sp"], 4, 4), ("sp", "tp_0", "tp_1"))
    in_specs = (
        P("sp", TP),
        P("sp", TP),
        P("sp"),
        P(None, TP),
        P("sp", TP),
        P(None, TP, None, None),
        P(None, TP, None, None),
        P(TP),
        P(TP, None),
        P(TP),
        P("sp", None),
        P("sp", None),
        P("sp", None, TP),
        P("sp", None, TP),
        P("sp", TP, None),
    )
    out_specs = P("sp", TP)
    return jax.shard_map(
        shards, mesh=split, in_specs=in_specs, out_specs=out_specs, check_vma=False
    )
```

```python
import jax
import jax.numpy as jnp
from jax import lax
from jax.experimental import pallas as pl
from jax.experimental.pallas import tpu as pltpu
from jax.sharding import Mesh
from jax.sharding import PartitionSpec as P

TP = ("tp_0", "tp_1")
INTERPRET = False

epsilon = 1e-06
f32 = jnp.float32
bf16 = jnp.bfloat16

BLOCKS = 32
PEERS = 16
ROWS = 64
GROUPS = 8
SLOTS = 5
PAD = 6
LINES = 10
LATER = 8
EROWS = BLOCKS * SLOTS
SENT = EROWS + 16

VMEM = pl.BlockSpec(memory_space=pltpu.VMEM)
SMEM = pl.BlockSpec(memory_space=pltpu.SMEM)
FAR = pl.BlockSpec(memory_space=pl.ANY if INTERPRET else pltpu.HBM)


def near(x):
    return x if INTERPRET else pltpu.with_memory_space_constraint(x, pltpu.VMEM)


def far(x):
    return x if INTERPRET else pltpu.with_memory_space_constraint(x, pltpu.HBM)


def call(body, in_specs, outs, scratch=(), copies=0, last=False):
    kept = jax.ShapeDtypeStruct if INTERPRET or last else pltpu.VMEM
    return pl.pallas_call(
        body,
        in_specs=in_specs,
        out_specs=[VMEM] * len(outs),
        out_shape=[kept(shape, dtype) for shape, dtype in outs],
        scratch_shapes=[
            (pltpu.SMEM if dtype == jnp.int32 else pltpu.VMEM)(shape, dtype)
            for shape, dtype in scratch
        ]
        + ([pltpu.SemaphoreType.DMA((copies,))] if copies else []),
        compiler_params=pltpu.CompilerParams(vmem_limit_bytes=16 * 2**20),
        interpret=INTERPRET,
    )


def iota(shape, dim):
    return lax.broadcasted_iota(jnp.int32, shape, dim)


def divided(x, by):
    return (x * (65536 // by + 1)) >> 16


def mm(a, b):
    return jnp.dot(a, b, preferred_element_type=f32)


def mm_across(a, b):
    return lax.dot_general(a, b, (((1,), (1,)), ((), ())), preferred_element_type=f32)


def halves_joined(first, second):
    left = iota((128, 128), 1) < 64
    return (
        jnp.where(left, first, pltpu.roll(second, 64, 1)),
        jnp.where(left, pltpu.roll(first, 64, 1), second),
    )


def steps_by_lane(log_step):
    eye = iota((GROUPS, GROUPS), 0) == iota((GROUPS, GROUPS), 1)
    step = jnp.exp(log_step)
    columns = [
        jnp.sum(
            jnp.where(eye, jnp.broadcast_to(step[k : k + 1, :], (GROUPS, GROUPS)), 0.0),
            axis=1,
            keepdims=True,
        )
        for k in range(2)
    ]
    return jnp.where(iota((GROUPS, 128), 1) < 64, columns[0], columns[1])


def one_minus_exp(x):
    series = jnp.ones_like(x)
    for n in range(9, 1, -1):
        series = 1.0 - x * (1.0 / n) * series
    return jnp.where(x < 0.5, x * series, 1.0 - jnp.exp(-x))


def sweep_body(
    me_ref, far_docs, far_step, far_extra, far_mix, *refs
):
    far_later, refs = refs[:LATER], refs[LATER:]
    message_ref, real_ref, imag_ref, keep_ref, turn_ref = refs[:5]
    later, refs = refs[5 : 5 + LATER], refs[5 + LATER :]
    masked, source, magnitude, log_step_ref, log_extra_ref, in_mix_ref, docs_ref, arrivals = refs
    x_ref = later[0]
    pairs = [
        (far_mix, in_mix_ref),
        (far_later[0], x_ref),
        (far_extra, log_extra_ref),
        (far_step, log_step_ref),
        (far_docs, docs_ref),
        *zip(far_later[1:], later[1:]),
    ]
    fetches = [
        pltpu.make_async_copy(distant, local, arrivals.at[k])
        for k, (distant, local) in enumerate(pairs)
    ]
    for fetch in fetches:
        fetch.start()
    for fetch in fetches[:5]:
        fetch.wait()
    lane = iota((GROUPS, 128), 1)
    fwd = lane < 64
    step = steps_by_lane(log_step_ref[...])
    theta = (jnp.pi * (lane & 63).astype(f32)) * step
    cos, sin = jnp.cos(theta), jnp.sin(theta)
    turn_ref[0] = cos
    turn_ref[1] = sin
    scale = jnp.sqrt(one_minus_exp(step))
    wide = iota((ROWS, 128), 1)
    x = x_ref[...].astype(f32)
    for g in range(GROUPS):
        masked[pl.ds(g, ROWS, stride=GROUPS), :] = jnp.where(wide // 16 == g, x, 0.0)
    log_extra = log_extra_ref[...]
    loss = -0.5 * step
    for n in range(ROWS):
        extra = jnp.broadcast_to(log_extra[:, n : n + 1], (GROUPS, 128))
        magnitude[pl.ds(GROUPS * n, GROUPS), :] = jnp.exp(loss + extra)
    mix_real, mix_imag = halves_joined(in_mix_ref[0], in_mix_ref[1])
    rows = masked[...].astype(bf16)
    source[0] = mm(rows, mix_real.astype(bf16))
    source[1] = mm(rows, mix_imag.astype(bf16))
    real = jnp.zeros((GROUPS, 128), f32)
    imag = jnp.zeros((GROUPS, 128), f32)
    total = jnp.ones((GROUPS, 128), f32)
    for n in range(ROWS):
        r = ROWS - 1 - n
        here, there = pl.ds(GROUPS * n, GROUPS), pl.ds(GROUPS * r, GROUPS)
        keep = jnp.where(fwd, magnitude[here, :], magnitude[there, :])
        if n > 0:
            same_fwd = jnp.where(docs_ref[n] == docs_ref[n - 1], 1.0, 0.0)
            same_bwd = jnp.where(docs_ref[r] == docs_ref[r + 1], 1.0, 0.0)
            keep = keep * jnp.where(fwd, same_fwd, same_bwd)
        new_real = scale * jnp.where(fwd, source[0, here, :], source[0, there, :])
        new_imag = scale * jnp.where(fwd, source[1, here, :], source[1, there, :])
        keep_ref[n] = keep
        real_ref[n] = new_real
        imag_ref[n] = new_imag
        by_cos, by_sin = keep * cos, keep * sin
        real, imag = (
            (by_cos * real + new_real) - by_sin * imag,
            (by_sin * real + new_imag) + by_cos * imag,
        )
        total = total * keep
    high = total.astype(bf16).astype(f32)
    low = total - high
    first_doc = docs_ref[0].astype(f32)
    last_doc = docs_ref[ROWS - 1].astype(f32)
    turn_ref[2] = jnp.where(fwd, first_doc, last_doc)
    group = iota((GROUPS, 128), 0)
    lines = []
    for kept, doc, left, right in [
        (0, last_doc, real, pltpu.roll(imag, 64, 1)),
        (64, first_doc, pltpu.roll(imag, 64, 1), real),
    ]:
        decays = jnp.where(lane == kept + group, high, 0.0) + jnp.where(
            lane == kept + GROUPS + group, low, 0.0
        )
        row = jnp.sum(decays, axis=0, keepdims=True) + jnp.where(
            lane[0:1] == kept + 2 * GROUPS, doc, 0.0
        )
        lines.append(jnp.where(fwd, left, right))
        lines.append(jnp.broadcast_to(row, (GROUPS, 128)))
    lines = jnp.concatenate(lines, axis=0).astype(bf16)
    row, entry = iota((BLOCKS * LINES, 32), 0), iota((BLOCKS * LINES, 32), 1)
    receiver = divided(row, LINES)
    wanted = row - receiver * LINES + jnp.where(receiver > me_ref[0], 0, 16)
    message_ref[...] = mm((entry == wanted).astype(f32).astype(bf16), lines).astype(bf16)
    for fetch in fetches[5:]:
        fetch.wait()


def mixer_body(
    me_ref, messages_ref, real_ref, imag_ref, keep_ref, turn_ref,
    x_ref, read_mix_ref, skip_ref, out_weight_ref,
    partial_ref,
    states, read_out, received, spread,
):
    lane = iota((GROUPS, 128), 1)
    fwd = lane < 64
    me = me_ref[0]
    cos, sin, mine = turn_ref[0], turn_ref[1], turn_ref[2]
    block_cos, block_sin = cos, sin
    for _ in range(6):
        block_cos, block_sin = (
            block_cos * block_cos - block_sin * block_sin,
            2.0 * block_cos * block_sin,
        )
    received[...] = messages_ref[...].astype(f32)
    place, group = lane & 63, iota((GROUPS, 128), 0)
    of_group = (place == group) | (place == GROUPS + group) | (place == 2 * GROUPS)
    scalars = jnp.concatenate(
        [
            jnp.where(of_group, received[LINES * n + GROUPS : LINES * n + GROUPS + 1, :], 0.0)
            for n in range(BLOCKS)
        ],
        axis=0,
    ).astype(bf16)
    entry = iota((128, 256), 0) & 63
    left = iota((128, 256), 1) < 128
    summed = (left & (entry < 2 * GROUPS)) | (~left & (entry == 2 * GROUPS))
    spread[...] = mm(scalars, summed.astype(f32).astype(bf16))
    real = jnp.zeros((GROUPS, 128), f32)
    imag = jnp.zeros((GROUPS, 128), f32)
    for n in range(BLOCKS - 1):
        r = BLOCKS - 1 - n
        one = received[LINES * n : LINES * n + GROUPS, :]
        two = received[LINES * r : LINES * r + GROUPS, :]
        here, there = pl.ds(GROUPS * n, GROUPS), pl.ds(GROUPS * r, GROUPS)
        decay = jnp.where(fwd, spread[here, 0:128], spread[there, 0:128])
        same = jnp.where(fwd, spread[here, 128:256], spread[there, 128:256]) == mine
        new_real = jnp.where(same, jnp.where(fwd, one, two), 0.0)
        new_imag = jnp.where(same, pltpu.roll(jnp.where(fwd, two, one), 64, 1), 0.0)
        by_cos, by_sin = decay * block_cos, decay * block_sin
        passed = jnp.where(fwd, (n < me).astype(jnp.int32), (r > me).astype(jnp.int32)) > 0
        real, imag = (
            jnp.where(passed, (by_cos * real + new_real) - by_sin * imag, real),
            jnp.where(passed, (by_sin * real + new_imag) + by_cos * imag, imag),
        )
    for n in range(ROWS):
        r = ROWS - 1 - n
        here, there = pl.ds(GROUPS * n, GROUPS), pl.ds(GROUPS * r, GROUPS)
        keep = keep_ref[n]
        by_cos, by_sin = keep * cos, keep * sin
        real, imag = (
            (by_cos * real + real_ref[n]) - by_sin * imag,
            (by_sin * real + imag_ref[n]) + by_cos * imag,
        )
        states[0, here, 0:64] = real[:, 0:64]
        states[0, there, 64:128] = real[:, 64:128]
        states[1, here, 0:64] = imag[:, 0:64]
        states[1, there, 64:128] = imag[:, 64:128]
    read_real, read_imag = halves_joined(read_mix_ref[0], read_mix_ref[1])
    read_out[...] = mm_across(states[0].astype(bf16), read_real.astype(bf16)) + mm_across(
        states[1].astype(bf16), read_imag.astype(bf16)
    )
    wide = iota((ROWS, 128), 1)
    mixed = skip_ref[...] * x_ref[...].astype(f32)
    for g in range(GROUPS):
        mixed = mixed + jnp.where(
            wide // 16 == g, read_out[pl.ds(g, ROWS, stride=GROUPS), :], 0.0
        )
    activated = jax.nn.gelu(mixed).astype(bf16)
    partial = mm(activated, out_weight_ref[...]).astype(bf16)
    for j in range(PEERS):
        partial_ref[j] = partial[:, 128 * j : 128 * (j + 1)]


def column(row):
    eye = iota((ROWS, ROWS), 0) == iota((ROWS, ROWS), 1)
    return jnp.sum(jnp.where(eye, row, 0.0), axis=1, keepdims=True)


def slots_down(routes, k):
    before = iota((ROWS, ROWS), 1) < iota((ROWS, ROWS), 0)
    expert = column(routes[k : k + 1])
    met = (expert == routes[0:1]).astype(f32) + (expert == routes[1:2]).astype(f32)
    rank = jnp.sum(jnp.where(before, met, 0.0), axis=1, keepdims=True)
    return expert * PAD + rank


def slots_across(routes, k):
    before = iota((ROWS, ROWS), 0) < iota((ROWS, ROWS), 1)
    expert = routes[k : k + 1]
    met = (column(routes[0:1]) == expert).astype(f32) + (column(routes[1:2]) == expert).astype(f32)
    rank = jnp.sum(jnp.where(before, met, 0.0), axis=0, keepdims=True)
    return expert * PAD + rank


def stream_body(arrived_ref, residual_ref, routes_ref, stream_ref, outgoing_ref):
    total = residual_ref[...].astype(f32)
    projected = arrived_ref[0].astype(f32)
    for j in range(1, PEERS):
        projected = projected + arrived_ref[j].astype(f32)
    stream = (total + projected).astype(bf16)
    stream_ref[...] = stream
    routes = routes_ref[...].astype(f32)
    slot = iota((BLOCKS * PAD, ROWS), 0).astype(f32)
    placing = (slot == slots_across(routes, 0)).astype(f32) + (
        slot == slots_across(routes, 1)
    ).astype(f32)
    outgoing_ref[...] = mm(placing.astype(bf16), stream).astype(bf16)


def packed_rows(shape, packed_dim):
    packed, padded = iota(shape, packed_dim), iota(shape, 1 - packed_dim)
    block = divided(padded, PAD)
    slot = padded - block * PAD
    return ((slot < SLOTS) & (packed == block * SLOTS + slot)).astype(f32).astype(bf16)


def copies_body(arrived_ref, gain_ref, copies_ref):
    rows = mm(packed_rows((EROWS, BLOCKS * PAD), 0), arrived_ref[...]).astype(bf16)
    gain = gain_ref[...]
    high = gain.astype(bf16).astype(f32)
    middle = (gain - high).astype(bf16).astype(f32)
    low = gain - high - middle
    row = iota((16, 128), 0)
    gains = jnp.where(
        row == 0, high, jnp.where(row == 1, middle, jnp.where(row == 2, low, 0.0))
    ).astype(bf16)
    for j in range(PEERS):
        copies_ref[j, 0:EROWS, :] = rows
        copies_ref[j, EROWS:SENT, :] = gains


def expert_body(rows_ref, gate_ref, up_ref, down_ref, terms_ref, normed):
    squares = jnp.zeros((EROWS, 128), f32)
    for j in range(PEERS):
        piece = rows_ref[j, 0:EROWS, :].astype(f32)
        squares = squares + piece * piece
    mean = jnp.sum(squares, axis=1, keepdims=True) / (128 * PEERS)
    factor = lax.rsqrt(mean + epsilon)
    for j in range(PEERS):
        gains = rows_ref[j, EROWS:SENT, :].astype(f32)
        gain = gains[0:1] + gains[1:2] + gains[2:3]
        piece = rows_ref[j, 0:EROWS, :].astype(f32)
        normed[:, 128 * j : 128 * (j + 1)] = (piece * factor * gain).astype(bf16)
    rows = normed[...]
    gate = mm(rows, gate_ref[0])
    up = mm(rows, up_ref[0])
    hidden = (jax.nn.silu(gate) * up).astype(bf16)
    terms = mm(hidden, down_ref[0]).astype(bf16)
    for j in range(PEERS):
        terms_ref[j] = terms[:, 128 * j : 128 * (j + 1)]


def answer_body(terms_ref, answer_ref):
    total = terms_ref[0].astype(f32)
    for j in range(1, PEERS):
        total = total + terms_ref[j].astype(f32)
    answer_ref[...] = mm(packed_rows((BLOCKS * PAD, EROWS), 1), total.astype(bf16)).astype(bf16)


def mixture_body(returned_ref, stream_ref, routes_ref, weight_ref, out_ref):
    routes, returned = routes_ref[...].astype(f32), returned_ref[...]
    slot = iota((ROWS, BLOCKS * PAD), 1).astype(f32)
    mixture = jnp.zeros((ROWS, 128), f32)
    for k in range(2):
        pick = (slot == slots_down(routes, k)).astype(f32).astype(bf16)
        mixture = mixture + mm(pick, returned) * column(weight_ref[k : k + 1, :])
    out_ref[...] = (stream_ref[...].astype(f32) + mixture).astype(bf16)


def exchanged(pieces, axis):
    return lax.all_to_all(pieces, axis, 0, 0, tiled=True)


def rows_exchanged(rows):
    pairs = rows.reshape(BLOCKS, rows.shape[0] // (2 * BLOCKS), 2, rows.shape[1])
    return exchanged(pairs, "sp").reshape(rows.shape)


def shards(
    mixer_in,
    residual,
    doc_ids,
    log_step,
    log_extra,
    in_mix,
    read_mix,
    skip_gain,
    out_weight,
    norm_gain,
    routes,
    route_weight,
    switch_matrices,
    up_weight,
    down_weight,
):
    me = lax.axis_index("sp").reshape(1)
    tall = GROUPS * ROWS
    later = (
        mixer_in,
        read_mix.swapaxes(2, 3).reshape(2, 128, 128),
        skip_gain.reshape(1, 128),
        out_weight,
        residual,
        routes.T,
        route_weight.T,
        norm_gain.reshape(1, 128),
    )
    message, real, imag, keep, turn, *later = call(
        sweep_body,
        [SMEM] + [FAR] * (4 + LATER),
        [
            ((BLOCKS * LINES, 128), bf16),
            ((ROWS, GROUPS, 128), f32),
            ((ROWS, GROUPS, 128), f32),
            ((ROWS, GROUPS, 128), f32),
            ((3, GROUPS, 128), f32),
            *((x.shape, x.dtype) for x in later),
        ],
        [
            ((tall, 128), f32),
            ((2, tall, 128), f32),
            ((tall, 128), f32),
            ((2, GROUPS), f32),
            ((GROUPS, ROWS), f32),
            ((2, 128, 128), f32),
            ((ROWS,), jnp.int32),
        ],
        copies=4 + LATER,
    )(
        me, far(doc_ids), far(log_step), far(log_extra.T), far(in_mix.reshape(2, 128, 128)),
        *map(far, later),
    )
    mixer_in, read_mix, skip_gain, out_weight, residual, routes, route_weight, norm_gain = map(
        near, later
    )
    messages = near(rows_exchanged(message))
    (partial,) = call(
        mixer_body,
        [SMEM] + [VMEM] * 9,
        [((PEERS, ROWS, 128), bf16)],
        [
            ((2, tall, 128), f32),
            ((tall, 128), f32),
            ((BLOCKS * LINES, 128), f32),
            ((BLOCKS * GROUPS, 256), f32),
        ],
    )(
        me, messages, near(real), near(imag), near(keep), near(turn),
        mixer_in, read_mix, skip_gain, out_weight,
    )
    shares = near(exchanged(partial, TP))
    stream, outgoing = call(
        stream_body,
        [VMEM] * 3,
        [((ROWS, 128), bf16), ((BLOCKS * PAD, 128), bf16)],
    )(shares, residual, routes)
    arrived = rows_exchanged(outgoing)
    (copies,) = call(copies_body, [VMEM] * 2, [((PEERS, SENT, 128), bf16)])(
        near(arrived), norm_gain
    )
    (terms,) = call(
        expert_body,
        [VMEM] * 4,
        [((PEERS, EROWS, 128), bf16)],
        [((EROWS, 128 * PEERS), bf16)],
    )(near(exchanged(copies, TP)), switch_matrices, up_weight, down_weight)
    (answer,) = call(answer_body, [VMEM], [((BLOCKS * PAD, 128), bf16)])(
        near(exchanged(terms, TP))
    )
    returned = rows_exchanged(answer)
    (out,) = call(mixture_body, [VMEM] * 4, [((ROWS, 128), bf16)], last=True)(
        near(returned), near(stream), routes, route_weight
    )
    return out


def solution(mesh):
    split = Mesh(mesh.devices.reshape(mesh.shape["sp"], 4, 4), ("sp", "tp_0", "tp_1"))
    in_specs = (
        P("sp", TP),
        P("sp", TP),
        P("sp"),
        P(None, TP),
        P("sp", TP),
        P(None, TP, None, None),
        P(None, TP, None, None),
        P(TP),
        P(TP, None),
        P(TP),
        P("sp", None),
        P("sp", None),
        P("sp", None, TP),
        P("sp", None, TP),
        P("sp", TP, None),
    )
    out_specs = P("sp", TP)
    return jax.shard_map(
        shards, mesh=split, in_specs=in_specs, out_specs=out_specs, check_vma=False
    )
```

```python
import jax
import jax.numpy as jnp
from jax import lax
from jax.experimental import pallas as pl
from jax.experimental.pallas import tpu as pltpu
from jax.sharding import Mesh
from jax.sharding import PartitionSpec as P

TP = ("tp_0", "tp_1")
INTERPRET = False

epsilon = 1e-06
f32 = jnp.float32
bf16 = jnp.bfloat16

BLOCKS = 32
PEERS = 16
ROWS = 64
GROUPS = 8
SLOTS = 5
PAD = 6
LINES = 10
SPANS = 4
SQUARED = 4
LATER = 8
EROWS = BLOCKS * SLOTS
SENT = EROWS + 4

VMEM = pl.BlockSpec(memory_space=pltpu.VMEM)
SMEM = pl.BlockSpec(memory_space=pltpu.SMEM)
FAR = pl.BlockSpec(memory_space=pl.ANY if INTERPRET else pltpu.HBM)


def near(x):
    return x if INTERPRET else pltpu.with_memory_space_constraint(x, pltpu.VMEM)


def far(x):
    return x if INTERPRET else pltpu.with_memory_space_constraint(x, pltpu.HBM)


def call(body, in_specs, outs, scratch=(), copies=0, last=False):
    kept = jax.ShapeDtypeStruct if INTERPRET or last else pltpu.VMEM
    return pl.pallas_call(
        body,
        in_specs=in_specs,
        out_specs=[VMEM] * len(outs),
        out_shape=[kept(shape, dtype) for shape, dtype in outs],
        scratch_shapes=[
            (pltpu.SMEM if dtype == jnp.int32 else pltpu.VMEM)(shape, dtype)
            for shape, dtype in scratch
        ]
        + ([pltpu.SemaphoreType.DMA((copies,))] if copies else []),
        compiler_params=pltpu.CompilerParams(vmem_limit_bytes=16 * 2**20),
        interpret=INTERPRET,
    )


def iota(shape, dim):
    return lax.broadcasted_iota(jnp.int32, shape, dim)


def divided(x, by):
    return (x * (65536 // by + 1)) >> 16


def mm(a, b):
    return jnp.dot(a, b, preferred_element_type=f32)


def mm_across(a, b):
    return lax.dot_general(a, b, (((1,), (1,)), ((), ())), preferred_element_type=f32)


def halves_joined(first, second):
    left = iota((128, 128), 1) < 64
    return (
        jnp.where(left, first, pltpu.roll(second, 64, 1)),
        jnp.where(left, pltpu.roll(first, 64, 1), second),
    )


def steps_by_lane(log_step):
    eye = iota((GROUPS, GROUPS), 0) == iota((GROUPS, GROUPS), 1)
    step = jnp.exp(log_step)
    columns = [
        jnp.sum(
            jnp.where(eye, jnp.broadcast_to(step[k : k + 1, :], (GROUPS, GROUPS)), 0.0),
            axis=1,
            keepdims=True,
        )
        for k in range(2)
    ]
    return jnp.where(iota((GROUPS, 128), 1) < 64, columns[0], columns[1])


def turned(by_cos, by_sin, real, imag, new_real, new_imag):
    return (
        (by_cos * real + new_real) - by_sin * imag,
        (by_sin * real + new_imag) + by_cos * imag,
    )


def raised(cos, sin, squarings):
    for _ in range(squarings):
        cos, sin = cos * cos - sin * sin, 2.0 * cos * sin
    return cos, sin


def one_minus_exp(x):
    series = jnp.ones_like(x)
    for n in range(9, 1, -1):
        series = 1.0 - x * (1.0 / n) * series
    return jnp.where(x < 0.5, x * series, 1.0 - jnp.exp(-x))


def sweep_body(
    me_ref, far_docs, far_step, far_extra, far_mix, *refs
):
    far_later, refs = refs[:LATER], refs[LATER:]
    message_ref, real_ref, imag_ref, keep_ref, turn_ref, span_ref = refs[:6]
    later, refs = refs[6 : 6 + LATER], refs[6 + LATER :]
    masked, source, magnitude, log_step_ref, log_extra_ref, in_mix_ref, docs_ref, arrivals = refs
    x_ref = later[0]
    pairs = [
        (far_step, log_step_ref),
        (far_extra, log_extra_ref),
        (far_docs, docs_ref),
        (far_later[0], x_ref),
        (far_mix, in_mix_ref),
        *zip(far_later[1:], later[1:]),
    ]
    fetches = [
        pltpu.make_async_copy(distant, local, arrivals.at[k])
        for k, (distant, local) in enumerate(pairs)
    ]
    for fetch in fetches:
        fetch.start()
    for fetch in fetches[:3]:
        fetch.wait()
    lane = iota((GROUPS, 128), 1)
    fwd = lane < 64
    step = steps_by_lane(log_step_ref[...])
    theta = (jnp.pi * (lane & 63).astype(f32)) * step
    cos, sin = jnp.cos(theta), jnp.sin(theta)
    turn_ref[0] = cos
    turn_ref[1] = sin
    scale = jnp.sqrt(one_minus_exp(step))
    log_extra = log_extra_ref[...]
    loss = -0.5 * step
    for n in range(ROWS):
        extra = jnp.broadcast_to(log_extra[:, n : n + 1], (GROUPS, 128))
        magnitude[pl.ds(GROUPS * n, GROUPS), :] = jnp.exp(loss + extra)
    for fetch in fetches[3:5]:
        fetch.wait()
    wide = iota((ROWS, 128), 1)
    x = x_ref[...].astype(f32)
    for g in range(GROUPS):
        masked[pl.ds(g, ROWS, stride=GROUPS), :] = jnp.where(wide // 16 == g, x, 0.0)
    mix_real, mix_imag = halves_joined(in_mix_ref[0], in_mix_ref[1])
    rows = masked[...].astype(bf16)
    source[0] = mm(rows, mix_real.astype(bf16))
    source[1] = mm(rows, mix_imag.astype(bf16))
    real = jnp.zeros((GROUPS, 128), f32)
    imag = jnp.zeros((GROUPS, 128), f32)
    total = jnp.ones((GROUPS, 128), f32)
    for n in range(ROWS):
        r = ROWS - 1 - n
        here, there = pl.ds(GROUPS * n, GROUPS), pl.ds(GROUPS * r, GROUPS)
        keep = jnp.where(fwd, magnitude[here, :], magnitude[there, :])
        if n > 0:
            same_fwd = jnp.where(docs_ref[n] == docs_ref[n - 1], 1.0, 0.0)
            same_bwd = jnp.where(docs_ref[r] == docs_ref[r + 1], 1.0, 0.0)
            keep = keep * jnp.where(fwd, same_fwd, same_bwd)
        new_real = scale * jnp.where(fwd, source[0, here, :], source[0, there, :])
        new_imag = scale * jnp.where(fwd, source[1, here, :], source[1, there, :])
        keep_ref[n] = keep
        real_ref[n] = new_real
        imag_ref[n] = new_imag
        by_cos, by_sin = keep * cos, keep * sin
        real, imag = (
            (by_cos * real + new_real) - by_sin * imag,
            (by_sin * real + new_imag) + by_cos * imag,
        )
        total = total * keep
        if (n + 1) % (ROWS // SPANS) == 0 and n + 1 < ROWS:
            for k, reached in enumerate((real, imag, total)):
                span_ref[n // (ROWS // SPANS), k] = reached
    high = total.astype(bf16).astype(f32)
    low = total - high
    first_doc = docs_ref[0].astype(f32)
    last_doc = docs_ref[ROWS - 1].astype(f32)
    turn_ref[2] = jnp.where(fwd, first_doc, last_doc)
    group = iota((GROUPS, 128), 0)
    lines = []
    for kept, doc, left, right in [
        (0, last_doc, real, pltpu.roll(imag, 64, 1)),
        (64, first_doc, pltpu.roll(imag, 64, 1), real),
    ]:
        decays = jnp.where(lane == kept + group, high, 0.0) + jnp.where(
            lane == kept + GROUPS + group, low, 0.0
        )
        row = jnp.sum(decays, axis=0, keepdims=True) + jnp.where(
            lane[0:1] == kept + 2 * GROUPS, doc, 0.0
        )
        lines.append(jnp.where(fwd, left, right))
        lines.append(jnp.broadcast_to(row, (GROUPS, 128)))
    lines = jnp.concatenate(lines, axis=0).astype(bf16)
    row, entry = iota((BLOCKS * LINES, 32), 0), iota((BLOCKS * LINES, 32), 1)
    receiver = divided(row, LINES)
    wanted = row - receiver * LINES + jnp.where(receiver > me_ref[0], 0, 16)
    message_ref[...] = mm((entry == wanted).astype(f32).astype(bf16), lines).astype(bf16)
    for fetch in fetches[5:]:
        fetch.wait()


def mixer_body(
    me_ref, messages_ref, real_ref, imag_ref, keep_ref, turn_ref, span_ref,
    x_ref, read_mix_ref, skip_ref, out_weight_ref,
    partial_ref,
    states, read_out, received, spread,
):
    lane = iota((GROUPS, 128), 1)
    fwd = lane < 64
    me = me_ref[0]
    cos, sin, mine = turn_ref[0], turn_ref[1], turn_ref[2]
    span_cos, span_sin = raised(cos, sin, SQUARED)
    block_cos, block_sin = raised(span_cos, span_sin, 6 - SQUARED)
    received[...] = messages_ref[...].astype(f32)
    place, group = lane & 63, iota((GROUPS, 128), 0)
    of_group = (place == group) | (place == GROUPS + group) | (place == 2 * GROUPS)
    scalars = jnp.concatenate(
        [
            jnp.where(of_group, received[LINES * n + GROUPS : LINES * n + GROUPS + 1, :], 0.0)
            for n in range(BLOCKS)
        ],
        axis=0,
    ).astype(bf16)
    entry = iota((128, 256), 0) & 63
    left = iota((128, 256), 1) < 128
    summed = (left & (entry < 2 * GROUPS)) | (~left & (entry == 2 * GROUPS))
    spread[...] = mm(scalars, summed.astype(f32).astype(bf16))
    real = jnp.zeros((GROUPS, 128), f32)
    imag = jnp.zeros((GROUPS, 128), f32)
    for n in range(BLOCKS - 1):
        r = BLOCKS - 1 - n
        one = received[LINES * n : LINES * n + GROUPS, :]
        two = received[LINES * r : LINES * r + GROUPS, :]
        here, there = pl.ds(GROUPS * n, GROUPS), pl.ds(GROUPS * r, GROUPS)
        decay = jnp.where(fwd, spread[here, 0:128], spread[there, 0:128])
        same = jnp.where(fwd, spread[here, 128:256], spread[there, 128:256]) == mine
        new_real = jnp.where(same, jnp.where(fwd, one, two), 0.0)
        new_imag = jnp.where(same, pltpu.roll(jnp.where(fwd, two, one), 64, 1), 0.0)
        by_cos, by_sin = decay * block_cos, decay * block_sin
        passed = jnp.where(fwd, (n < me).astype(jnp.int32), (r > me).astype(jnp.int32)) > 0
        real, imag = (
            jnp.where(passed, (by_cos * real + new_real) - by_sin * imag, real),
            jnp.where(passed, (by_sin * real + new_imag) + by_cos * imag, imag),
        )
    span = ROWS // SPANS
    parts = [(real, imag)]
    far_cos, far_sin = span_cos, span_sin
    for q in range(SPANS - 1):
        total = span_ref[q, 2]
        parts.append(
            turned(total * far_cos, total * far_sin, real, imag, span_ref[q, 0], span_ref[q, 1])
        )
        far_cos, far_sin = (
            far_cos * span_cos - far_sin * span_sin,
            far_cos * span_sin + far_sin * span_cos,
        )
    for m in range(span):
        for q in range(SPANS):
            n = span * q + m
            r = ROWS - 1 - n
            here, there = pl.ds(GROUPS * n, GROUPS), pl.ds(GROUPS * r, GROUPS)
            keep = keep_ref[n]
            parts[q] = turned(keep * cos, keep * sin, *parts[q], real_ref[n], imag_ref[n])
            states[0, here, 0:64] = parts[q][0][:, 0:64]
            states[0, there, 64:128] = parts[q][0][:, 64:128]
            states[1, here, 0:64] = parts[q][1][:, 0:64]
            states[1, there, 64:128] = parts[q][1][:, 64:128]
    read_real, read_imag = halves_joined(read_mix_ref[0], read_mix_ref[1])
    read_out[...] = mm_across(states[0].astype(bf16), read_real.astype(bf16)) + mm_across(
        states[1].astype(bf16), read_imag.astype(bf16)
    )
    wide = iota((ROWS, 128), 1)
    mixed = skip_ref[...] * x_ref[...].astype(f32)
    for g in range(GROUPS):
        mixed = mixed + jnp.where(
            wide // 16 == g, read_out[pl.ds(g, ROWS, stride=GROUPS), :], 0.0
        )
    activated = jax.nn.gelu(mixed).astype(bf16)
    partial = mm(activated, out_weight_ref[...]).astype(bf16)
    for j in range(PEERS):
        partial_ref[j] = partial[:, 128 * j : 128 * (j + 1)]


def column(row):
    eye = iota((ROWS, ROWS), 0) == iota((ROWS, ROWS), 1)
    return jnp.sum(jnp.where(eye, row, 0.0), axis=1, keepdims=True)


def slots_down(routes, k):
    before = iota((ROWS, ROWS), 1) < iota((ROWS, ROWS), 0)
    expert = column(routes[k : k + 1])
    met = (expert == routes[0:1]).astype(f32) + (expert == routes[1:2]).astype(f32)
    rank = jnp.sum(jnp.where(before, met, 0.0), axis=1, keepdims=True)
    return expert * PAD + rank


def slots_across(routes, k):
    before = iota((ROWS, ROWS), 0) < iota((ROWS, ROWS), 1)
    expert = routes[k : k + 1]
    met = (column(routes[0:1]) == expert).astype(f32) + (column(routes[1:2]) == expert).astype(f32)
    rank = jnp.sum(jnp.where(before, met, 0.0), axis=0, keepdims=True)
    return expert * PAD + rank


def stream_body(arrived_ref, residual_ref, routes_ref, stream_ref, outgoing_ref):
    total = residual_ref[...].astype(f32)
    projected = arrived_ref[0].astype(f32)
    for j in range(1, PEERS):
        projected = projected + arrived_ref[j].astype(f32)
    stream = (total + projected).astype(bf16)
    stream_ref[...] = stream
    routes = routes_ref[...].astype(f32)
    slot = iota((BLOCKS * PAD, ROWS), 0).astype(f32)
    placing = (slot == slots_across(routes, 0)).astype(f32) + (
        slot == slots_across(routes, 1)
    ).astype(f32)
    outgoing_ref[...] = mm(placing.astype(bf16), stream).astype(bf16)


def packed_rows(shape, packed_dim):
    packed, padded = iota(shape, packed_dim), iota(shape, 1 - packed_dim)
    block = divided(padded, PAD)
    slot = padded - block * PAD
    return ((slot < SLOTS) & (packed == block * SLOTS + slot)).astype(f32).astype(bf16)


def copies_body(arrived_ref, gain_ref, copies_ref):
    row = iota((2 * SENT, BLOCKS * PAD), 0)
    row = jnp.where(row >= SENT, row - SENT, row)
    padded = iota((2 * SENT, BLOCKS * PAD), 1)
    block = divided(padded, PAD)
    slot = padded - block * PAD
    packing = (slot < SLOTS) & (row == block * SLOTS + slot)
    rows = mm(packing.astype(f32).astype(bf16), arrived_ref[...])
    gain = gain_ref[...]
    high = gain.astype(bf16).astype(f32)
    middle = (gain - high).astype(bf16).astype(f32)
    low = gain - high - middle
    row = iota((2 * SENT, 128), 0)
    row = jnp.where(row >= SENT, row - SENT, row) - EROWS
    for k, part in enumerate((high, middle, low)):
        rows = jnp.where(row == k, part, rows)
    rows = rows.astype(bf16)
    for j in range(PEERS // 2):
        copies_ref[j] = rows


def expert_body(rows_ref, gate_ref, up_ref, down_ref, terms_ref, normed, pieces):
    squares = jnp.zeros((EROWS, 128), f32)
    for j in range(PEERS // 2):
        pieces[j] = rows_ref[j].astype(f32)
    starts = [(j // 2, SENT * (j % 2)) for j in range(PEERS)]
    for block, start in starts:
        piece = pieces[block, start : start + EROWS, :]
        squares = squares + piece * piece
    mean = jnp.sum(squares, axis=1, keepdims=True) / (128 * PEERS)
    factor = lax.rsqrt(mean + epsilon)
    for j, (block, start) in enumerate(starts):
        end = start + EROWS
        gain = (
            pieces[block, end : end + 1, :]
            + pieces[block, end + 1 : end + 2, :]
            + pieces[block, end + 2 : end + 3, :]
        )
        piece = pieces[block, start:end, :]
        normed[:, 128 * j : 128 * (j + 1)] = (piece * factor * gain).astype(bf16)
    rows = normed[...]
    gate = mm(rows, gate_ref[0])
    up = mm(rows, up_ref[0])
    hidden = (jax.nn.silu(gate) * up).astype(bf16)
    terms = mm(hidden, down_ref[0]).astype(bf16)
    for j in range(PEERS):
        terms_ref[j] = terms[:, 128 * j : 128 * (j + 1)]


def answer_body(terms_ref, answer_ref):
    total = terms_ref[0].astype(f32)
    for j in range(1, PEERS):
        total = total + terms_ref[j].astype(f32)
    answer_ref[...] = mm(packed_rows((BLOCKS * PAD, EROWS), 1), total.astype(bf16)).astype(bf16)


def mixture_body(returned_ref, stream_ref, routes_ref, weight_ref, out_ref):
    routes, returned = routes_ref[...].astype(f32), returned_ref[...]
    slot = iota((ROWS, BLOCKS * PAD), 1).astype(f32)
    mixture = jnp.zeros((ROWS, 128), f32)
    for k in range(2):
        pick = (slot == slots_down(routes, k)).astype(f32).astype(bf16)
        mixture = mixture + mm(pick, returned) * column(weight_ref[k : k + 1, :])
    out_ref[...] = (stream_ref[...].astype(f32) + mixture).astype(bf16)


def exchanged(pieces, axis):
    return lax.all_to_all(pieces, axis, 0, 0, tiled=True)


def rows_exchanged(rows):
    pairs = rows.reshape(BLOCKS, rows.shape[0] // (2 * BLOCKS), 2, rows.shape[1])
    return exchanged(pairs, "sp").reshape(rows.shape)


def shards(
    mixer_in,
    residual,
    doc_ids,
    log_step,
    log_extra,
    in_mix,
    read_mix,
    skip_gain,
    out_weight,
    norm_gain,
    routes,
    route_weight,
    switch_matrices,
    up_weight,
    down_weight,
):
    me = lax.axis_index("sp").reshape(1)
    tall = GROUPS * ROWS
    later = (
        mixer_in,
        read_mix.swapaxes(2, 3).reshape(2, 128, 128),
        skip_gain.reshape(1, 128),
        out_weight,
        residual,
        routes.T,
        route_weight.T,
        norm_gain.reshape(1, 128),
    )
    message, real, imag, keep, turn, span, *later = call(
        sweep_body,
        [SMEM] + [FAR] * (4 + LATER),
        [
            ((BLOCKS * LINES, 128), bf16),
            ((ROWS, GROUPS, 128), f32),
            ((ROWS, GROUPS, 128), f32),
            ((ROWS, GROUPS, 128), f32),
            ((3, GROUPS, 128), f32),
            ((SPANS - 1, 3, GROUPS, 128), f32),
            *((x.shape, x.dtype) for x in later),
        ],
        [
            ((tall, 128), f32),
            ((2, tall, 128), f32),
            ((tall, 128), f32),
            ((2, GROUPS), f32),
            ((GROUPS, ROWS), f32),
            ((2, 128, 128), f32),
            ((ROWS,), jnp.int32),
        ],
        copies=4 + LATER,
    )(
        me, far(doc_ids), far(log_step), far(log_extra.T), far(in_mix.reshape(2, 128, 128)),
        *map(far, later),
    )
    mixer_in, read_mix, skip_gain, out_weight, residual, routes, route_weight, norm_gain = map(
        near, later
    )
    messages = near(rows_exchanged(message))
    (partial,) = call(
        mixer_body,
        [SMEM] + [VMEM] * 10,
        [((PEERS, ROWS, 128), bf16)],
        [
            ((2, tall, 128), f32),
            ((tall, 128), f32),
            ((BLOCKS * LINES, 128), f32),
            ((BLOCKS * GROUPS, 256), f32),
        ],
    )(
        me, messages, near(real), near(imag), near(keep), near(turn), near(span),
        mixer_in, read_mix, skip_gain, out_weight,
    )
    shares = near(exchanged(partial, TP))
    stream, outgoing = call(
        stream_body,
        [VMEM] * 3,
        [((ROWS, 128), bf16), ((BLOCKS * PAD, 128), bf16)],
    )(shares, residual, routes)
    arrived = rows_exchanged(outgoing)
    (copies,) = call(copies_body, [VMEM] * 2, [((PEERS // 2, 2 * SENT, 128), bf16)])(
        near(arrived), norm_gain
    )
    gathered = exchanged(copies.reshape(PEERS, SENT // 2, 2, 128), TP).reshape(copies.shape)
    (terms,) = call(
        expert_body,
        [VMEM] * 4,
        [((PEERS, EROWS, 128), bf16)],
        [((EROWS, 128 * PEERS), bf16), ((PEERS // 2, 2 * SENT, 128), f32)],
    )(near(gathered), switch_matrices, up_weight, down_weight)
    (answer,) = call(answer_body, [VMEM], [((BLOCKS * PAD, 128), bf16)])(
        near(exchanged(terms, TP))
    )
    returned = rows_exchanged(answer)
    (out,) = call(mixture_body, [VMEM] * 4, [((ROWS, 128), bf16)], last=True)(
        near(returned), near(stream), routes, route_weight
    )
    return out


def solution(mesh):
    split = Mesh(mesh.devices.reshape(mesh.shape["sp"], 4, 4), ("sp", "tp_0", "tp_1"))
    in_specs = (
        P("sp", TP),
        P("sp", TP),
        P("sp"),
        P(None, TP),
        P("sp", TP),
        P(None, TP, None, None),
        P(None, TP, None, None),
        P(TP),
        P(TP, None),
        P(TP),
        P("sp", None),
        P("sp", None),
        P("sp", None, TP),
        P("sp", None, TP),
        P("sp", TP, None),
    )
    out_specs = P("sp", TP)
    return jax.shard_map(
        shards, mesh=split, in_specs=in_specs, out_specs=out_specs, check_vma=False
    )
```

```python
import jax
import jax.numpy as jnp
from jax import lax
from jax.experimental import pallas as pl
from jax.experimental.pallas import tpu as pltpu
from jax.sharding import Mesh
from jax.sharding import PartitionSpec as P

TP = ("tp_0", "tp_1")
INTERPRET = False

epsilon = 1e-06
f32 = jnp.float32
bf16 = jnp.bfloat16

BLOCKS = 32
PEERS = 16
ROWS = 64
GROUPS = 8
SLOTS = 5
PAD = 6
LINES = 10
SPANS = 4
SQUARED = 4
LATER = 8
EROWS = BLOCKS * SLOTS
SENT = EROWS + 4

VMEM = pl.BlockSpec(memory_space=pltpu.VMEM)
FAR = pl.BlockSpec(memory_space=pl.ANY if INTERPRET else pltpu.HBM)


def near(x):
    return x if INTERPRET else pltpu.with_memory_space_constraint(x, pltpu.VMEM)


def far(x):
    return x if INTERPRET else pltpu.with_memory_space_constraint(x, pltpu.HBM)


def call(body, in_specs, outs, scratch=(), copies=0, last=False):
    kept = jax.ShapeDtypeStruct if INTERPRET or last else pltpu.VMEM
    return pl.pallas_call(
        body,
        in_specs=in_specs,
        out_specs=[VMEM] * len(outs),
        out_shape=[kept(shape, dtype) for shape, dtype in outs],
        scratch_shapes=[
            (pltpu.SMEM if dtype == jnp.int32 else pltpu.VMEM)(shape, dtype)
            for shape, dtype in scratch
        ]
        + ([pltpu.SemaphoreType.DMA((copies,))] if copies else []),
        compiler_params=pltpu.CompilerParams(vmem_limit_bytes=16 * 2**20),
        interpret=INTERPRET,
    )


def iota(shape, dim):
    return lax.broadcasted_iota(jnp.int32, shape, dim)


def divided(x, by):
    return (x * (65536 // by + 1)) >> 16


def mm(a, b):
    return jnp.dot(a, b, preferred_element_type=f32)


def mm_across(a, b):
    return lax.dot_general(a, b, (((1,), (1,)), ((), ())), preferred_element_type=f32)


def halves_joined(first, second):
    left = iota((128, 128), 1) < 64
    return (
        jnp.where(left, first, pltpu.roll(second, 64, 1)),
        jnp.where(left, pltpu.roll(first, 64, 1), second),
    )


def steps_by_lane(log_step):
    eye = iota((GROUPS, GROUPS), 0) == iota((GROUPS, GROUPS), 1)
    step = jnp.exp(log_step)
    columns = [
        jnp.sum(
            jnp.where(eye, jnp.broadcast_to(step[k : k + 1, :], (GROUPS, GROUPS)), 0.0),
            axis=1,
            keepdims=True,
        )
        for k in range(2)
    ]
    return jnp.where(iota((GROUPS, 128), 1) < 64, columns[0], columns[1])


def turned(by_cos, by_sin, real, imag, new_real, new_imag):
    return (
        (by_cos * real + new_real) - by_sin * imag,
        (by_sin * real + new_imag) + by_cos * imag,
    )


def raised(cos, sin, squarings):
    for _ in range(squarings):
        cos, sin = cos * cos - sin * sin, 2.0 * cos * sin
    return cos, sin


def one_minus_exp(x):
    series = jnp.ones_like(x)
    for n in range(9, 1, -1):
        series = 1.0 - x * (1.0 / n) * series
    return jnp.where(x < 0.5, x * series, 1.0 - jnp.exp(-x))


def sweep_body(
    far_me, far_docs, far_step, far_extra, far_mix, *refs
):
    far_later, refs = refs[:LATER], refs[LATER:]
    message_ref, real_ref, imag_ref, keep_ref, turn_ref, span_ref = refs[:6]
    later, refs = refs[6 : 6 + LATER], refs[6 + LATER :]
    masked, source, magnitude, log_step_ref, log_extra_ref, in_mix_ref, docs_ref, me_ref, arrivals = (
        refs
    )
    x_ref = later[0]
    pairs = [
        (far_step, log_step_ref),
        (far_extra, log_extra_ref),
        (far_docs, docs_ref),
        (far_me, me_ref),
        (far_later[0], x_ref),
        (far_mix, in_mix_ref),
        *zip(far_later[1:], later[1:]),
    ]
    fetches = [
        pltpu.make_async_copy(distant, local, arrivals.at[k])
        for k, (distant, local) in enumerate(pairs)
    ]
    for fetch in fetches:
        fetch.start()
    for fetch in fetches[:4]:
        fetch.wait()
    lane = iota((GROUPS, 128), 1)
    fwd = lane < 64
    step = steps_by_lane(log_step_ref[...])
    theta = (jnp.pi * (lane & 63).astype(f32)) * step
    cos, sin = jnp.cos(theta), jnp.sin(theta)
    turn_ref[0] = cos
    turn_ref[1] = sin
    scale = jnp.sqrt(one_minus_exp(step))
    log_extra = log_extra_ref[...]
    loss = -0.5 * step
    for n in range(ROWS):
        extra = jnp.broadcast_to(log_extra[:, n : n + 1], (GROUPS, 128))
        magnitude[pl.ds(GROUPS * n, GROUPS), :] = jnp.exp(loss + extra)
    for fetch in fetches[4:6]:
        fetch.wait()
    wide = iota((ROWS, 128), 1)
    x = x_ref[...].astype(f32)
    for g in range(GROUPS):
        masked[pl.ds(g, ROWS, stride=GROUPS), :] = jnp.where(wide // 16 == g, x, 0.0)
    mix_real, mix_imag = halves_joined(in_mix_ref[0], in_mix_ref[1])
    rows = masked[...].astype(bf16)
    source[0] = mm(rows, mix_real.astype(bf16))
    source[1] = mm(rows, mix_imag.astype(bf16))
    real = jnp.zeros((GROUPS, 128), f32)
    imag = jnp.zeros((GROUPS, 128), f32)
    total = jnp.ones((GROUPS, 128), f32)
    for n in range(ROWS):
        r = ROWS - 1 - n
        here, there = pl.ds(GROUPS * n, GROUPS), pl.ds(GROUPS * r, GROUPS)
        keep = jnp.where(fwd, magnitude[here, :], magnitude[there, :])
        if n > 0:
            same_fwd = jnp.where(docs_ref[n] == docs_ref[n - 1], 1.0, 0.0)
            same_bwd = jnp.where(docs_ref[r] == docs_ref[r + 1], 1.0, 0.0)
            keep = keep * jnp.where(fwd, same_fwd, same_bwd)
        new_real = scale * jnp.where(fwd, source[0, here, :], source[0, there, :])
        new_imag = scale * jnp.where(fwd, source[1, here, :], source[1, there, :])
        keep_ref[n] = keep
        real_ref[n] = new_real
        imag_ref[n] = new_imag
        by_cos, by_sin = keep * cos, keep * sin
        real, imag = (
            (by_cos * real + new_real) - by_sin * imag,
            (by_sin * real + new_imag) + by_cos * imag,
        )
        total = total * keep
        if (n + 1) % (ROWS // SPANS) == 0 and n + 1 < ROWS:
            for k, reached in enumerate((real, imag, total)):
                span_ref[n // (ROWS // SPANS), k] = reached
    high = total.astype(bf16).astype(f32)
    low = total - high
    first_doc = docs_ref[0].astype(f32)
    last_doc = docs_ref[ROWS - 1].astype(f32)
    turn_ref[2] = jnp.where(fwd, first_doc, last_doc)
    turn_ref[3] = jnp.broadcast_to(me_ref[0].astype(f32), (GROUPS, 128))
    group = iota((GROUPS, 128), 0)
    lines = []
    for kept, doc, left, right in [
        (0, last_doc, real, pltpu.roll(imag, 64, 1)),
        (64, first_doc, pltpu.roll(imag, 64, 1), real),
    ]:
        decays = jnp.where(lane == kept + group, high, 0.0) + jnp.where(
            lane == kept + GROUPS + group, low, 0.0
        )
        row = jnp.sum(decays, axis=0, keepdims=True) + jnp.where(
            lane[0:1] == kept + 2 * GROUPS, doc, 0.0
        )
        lines.append(jnp.where(fwd, left, right))
        lines.append(jnp.broadcast_to(row, (GROUPS, 128)))
    lines = jnp.concatenate(lines, axis=0).astype(bf16)
    row, entry = iota((BLOCKS * LINES, 32), 0), iota((BLOCKS * LINES, 32), 1)
    receiver = divided(row, LINES)
    wanted = row - receiver * LINES + jnp.where(receiver > me_ref[0], 0, 16)
    message_ref[...] = mm((entry == wanted).astype(f32).astype(bf16), lines).astype(bf16)
    for fetch in fetches[6:]:
        fetch.wait()


def mixer_body(
    messages_ref, real_ref, imag_ref, keep_ref, turn_ref, span_ref,
    x_ref, read_mix_ref, skip_ref, out_weight_ref,
    partial_ref,
    states, read_out, received, spread,
):
    lane = iota((GROUPS, 128), 1)
    fwd = lane < 64
    cos, sin, mine, me = turn_ref[0], turn_ref[1], turn_ref[2], turn_ref[3]
    span_cos, span_sin = raised(cos, sin, SQUARED)
    block_cos, block_sin = raised(span_cos, span_sin, 6 - SQUARED)
    received[...] = messages_ref[...].astype(f32)
    place, group = lane & 63, iota((GROUPS, 128), 0)
    of_group = (place == group) | (place == GROUPS + group) | (place == 2 * GROUPS)
    scalars = jnp.concatenate(
        [
            jnp.where(of_group, received[LINES * n + GROUPS : LINES * n + GROUPS + 1, :], 0.0)
            for n in range(BLOCKS)
        ],
        axis=0,
    ).astype(bf16)
    entry = iota((128, 256), 0) & 63
    left = iota((128, 256), 1) < 128
    summed = (left & (entry < 2 * GROUPS)) | (~left & (entry == 2 * GROUPS))
    spread[...] = mm(scalars, summed.astype(f32).astype(bf16))
    real = jnp.zeros((GROUPS, 128), f32)
    imag = jnp.zeros((GROUPS, 128), f32)
    for n in range(BLOCKS - 1):
        r = BLOCKS - 1 - n
        one = received[LINES * n : LINES * n + GROUPS, :]
        two = received[LINES * r : LINES * r + GROUPS, :]
        here, there = pl.ds(GROUPS * n, GROUPS), pl.ds(GROUPS * r, GROUPS)
        decay = jnp.where(fwd, spread[here, 0:128], spread[there, 0:128])
        same = jnp.where(fwd, spread[here, 128:256], spread[there, 128:256]) == mine
        new_real = jnp.where(same, jnp.where(fwd, one, two), 0.0)
        new_imag = jnp.where(same, pltpu.roll(jnp.where(fwd, two, one), 64, 1), 0.0)
        by_cos, by_sin = decay * block_cos, decay * block_sin
        passed = (fwd & (me > n)) | (~fwd & (me < r))
        real, imag = (
            jnp.where(passed, (by_cos * real + new_real) - by_sin * imag, real),
            jnp.where(passed, (by_sin * real + new_imag) + by_cos * imag, imag),
        )
    span = ROWS // SPANS
    parts = [(real, imag)]
    far_cos, far_sin = span_cos, span_sin
    for q in range(SPANS - 1):
        total = span_ref[q, 2]
        parts.append(
            turned(total * far_cos, total * far_sin, real, imag, span_ref[q, 0], span_ref[q, 1])
        )
        far_cos, far_sin = (
            far_cos * span_cos - far_sin * span_sin,
            far_cos * span_sin + far_sin * span_cos,
        )
    for m in range(span):
        for q in range(SPANS):
            n = span * q + m
            r = ROWS - 1 - n
            here, there = pl.ds(GROUPS * n, GROUPS), pl.ds(GROUPS * r, GROUPS)
            keep = keep_ref[n]
            parts[q] = turned(keep * cos, keep * sin, *parts[q], real_ref[n], imag_ref[n])
            states[0, here, 0:64] = parts[q][0][:, 0:64]
            states[0, there, 64:128] = parts[q][0][:, 64:128]
            states[1, here, 0:64] = parts[q][1][:, 0:64]
            states[1, there, 64:128] = parts[q][1][:, 64:128]
    read_real, read_imag = halves_joined(read_mix_ref[0], read_mix_ref[1])
    read_out[...] = mm_across(states[0].astype(bf16), read_real.astype(bf16)) + mm_across(
        states[1].astype(bf16), read_imag.astype(bf16)
    )
    wide = iota((ROWS, 128), 1)
    mixed = skip_ref[...] * x_ref[...].astype(f32)
    for g in range(GROUPS):
        mixed = mixed + jnp.where(
            wide // 16 == g, read_out[pl.ds(g, ROWS, stride=GROUPS), :], 0.0
        )
    activated = jax.nn.gelu(mixed).astype(bf16)
    partial = mm(activated, out_weight_ref[...]).astype(bf16)
    for j in range(PEERS):
        partial_ref[j] = partial[:, 128 * j : 128 * (j + 1)]


def column(row):
    eye = iota((ROWS, ROWS), 0) == iota((ROWS, ROWS), 1)
    return jnp.sum(jnp.where(eye, row, 0.0), axis=1, keepdims=True)


def slots_down(routes, k):
    before = iota((ROWS, ROWS), 1) < iota((ROWS, ROWS), 0)
    expert = column(routes[k : k + 1])
    met = (expert == routes[0:1]).astype(f32) + (expert == routes[1:2]).astype(f32)
    rank = jnp.sum(jnp.where(before, met, 0.0), axis=1, keepdims=True)
    return expert * PAD + rank


def slots_across(routes, k):
    before = iota((ROWS, ROWS), 0) < iota((ROWS, ROWS), 1)
    expert = routes[k : k + 1]
    met = (column(routes[0:1]) == expert).astype(f32) + (column(routes[1:2]) == expert).astype(f32)
    rank = jnp.sum(jnp.where(before, met, 0.0), axis=0, keepdims=True)
    return expert * PAD + rank


def stream_body(arrived_ref, residual_ref, routes_ref, stream_ref, outgoing_ref):
    total = residual_ref[...].astype(f32)
    projected = arrived_ref[0].astype(f32)
    for j in range(1, PEERS):
        projected = projected + arrived_ref[j].astype(f32)
    stream = (total + projected).astype(bf16)
    stream_ref[...] = stream
    routes = routes_ref[...].astype(f32)
    slot = iota((BLOCKS * PAD, ROWS), 0).astype(f32)
    placing = (slot == slots_across(routes, 0)).astype(f32) + (
        slot == slots_across(routes, 1)
    ).astype(f32)
    outgoing_ref[...] = mm(placing.astype(bf16), stream).astype(bf16)


def packed_rows(shape, packed_dim):
    packed, padded = iota(shape, packed_dim), iota(shape, 1 - packed_dim)
    block = divided(padded, PAD)
    slot = padded - block * PAD
    return ((slot < SLOTS) & (packed == block * SLOTS + slot)).astype(f32).astype(bf16)


def copies_body(arrived_ref, gain_ref, copies_ref):
    row = iota((2 * SENT, BLOCKS * PAD), 0)
    row = jnp.where(row >= SENT, row - SENT, row)
    padded = iota((2 * SENT, BLOCKS * PAD), 1)
    block = divided(padded, PAD)
    slot = padded - block * PAD
    packing = (slot < SLOTS) & (row == block * SLOTS + slot)
    rows = mm(packing.astype(f32).astype(bf16), arrived_ref[...])
    gain = gain_ref[...]
    high = gain.astype(bf16).astype(f32)
    middle = (gain - high).astype(bf16).astype(f32)
    low = gain - high - middle
    row = iota((2 * SENT, 128), 0)
    row = jnp.where(row >= SENT, row - SENT, row) - EROWS
    for k, part in enumerate((high, middle, low)):
        rows = jnp.where(row == k, part, rows)
    rows = rows.astype(bf16)
    for j in range(PEERS // 2):
        copies_ref[j] = rows


def expert_body(rows_ref, gate_ref, up_ref, down_ref, terms_ref, normed, pieces):
    squares = jnp.zeros((EROWS, 128), f32)
    for j in range(PEERS // 2):
        pieces[j] = rows_ref[j].astype(f32)
    starts = [(j // 2, SENT * (j % 2)) for j in range(PEERS)]
    for block, start in starts:
        piece = pieces[block, start : start + EROWS, :]
        squares = squares + piece * piece
    mean = jnp.sum(squares, axis=1, keepdims=True) / (128 * PEERS)
    factor = lax.rsqrt(mean + epsilon)
    for j, (block, start) in enumerate(starts):
        end = start + EROWS
        gain = (
            pieces[block, end : end + 1, :]
            + pieces[block, end + 1 : end + 2, :]
            + pieces[block, end + 2 : end + 3, :]
        )
        piece = pieces[block, start:end, :]
        normed[:, 128 * j : 128 * (j + 1)] = (piece * factor * gain).astype(bf16)
    rows = normed[...]
    gate = mm(rows, gate_ref[0])
    up = mm(rows, up_ref[0])
    hidden = (jax.nn.silu(gate) * up).astype(bf16)
    terms = mm(hidden, down_ref[0]).astype(bf16)
    for j in range(PEERS):
        terms_ref[j] = terms[:, 128 * j : 128 * (j + 1)]


def answer_body(terms_ref, answer_ref):
    total = terms_ref[0].astype(f32)
    for j in range(1, PEERS):
        total = total + terms_ref[j].astype(f32)
    answer_ref[...] = mm(packed_rows((BLOCKS * PAD, EROWS), 1), total.astype(bf16)).astype(bf16)


def mixture_body(returned_ref, stream_ref, routes_ref, weight_ref, out_ref):
    routes, returned = routes_ref[...].astype(f32), returned_ref[...]
    slot = iota((ROWS, BLOCKS * PAD), 1).astype(f32)
    mixture = jnp.zeros((ROWS, 128), f32)
    for k in range(2):
        pick = (slot == slots_down(routes, k)).astype(f32).astype(bf16)
        mixture = mixture + mm(pick, returned) * column(weight_ref[k : k + 1, :])
    out_ref[...] = (stream_ref[...].astype(f32) + mixture).astype(bf16)


def exchanged(pieces, axis):
    return lax.all_to_all(pieces, axis, 0, 0, tiled=True)


def rows_exchanged(rows):
    pairs = rows.reshape(BLOCKS, rows.shape[0] // (2 * BLOCKS), 2, rows.shape[1])
    return exchanged(pairs, "sp").reshape(rows.shape)


def shards(
    mixer_in,
    residual,
    doc_ids,
    log_step,
    log_extra,
    in_mix,
    read_mix,
    skip_gain,
    out_weight,
    norm_gain,
    routes,
    route_weight,
    switch_matrices,
    up_weight,
    down_weight,
):
    me = lax.axis_index("sp").reshape(1)
    tall = GROUPS * ROWS
    later = (
        mixer_in,
        read_mix.swapaxes(2, 3).reshape(2, 128, 128),
        skip_gain.reshape(1, 128),
        out_weight,
        residual,
        routes.T,
        route_weight.T,
        norm_gain.reshape(1, 128),
    )
    message, real, imag, keep, turn, span, *later = call(
        sweep_body,
        [FAR] * (5 + LATER),
        [
            ((BLOCKS * LINES, 128), bf16),
            ((ROWS, GROUPS, 128), f32),
            ((ROWS, GROUPS, 128), f32),
            ((ROWS, GROUPS, 128), f32),
            ((4, GROUPS, 128), f32),
            ((SPANS - 1, 3, GROUPS, 128), f32),
            *((x.shape, x.dtype) for x in later),
        ],
        [
            ((tall, 128), f32),
            ((2, tall, 128), f32),
            ((tall, 128), f32),
            ((2, GROUPS), f32),
            ((GROUPS, ROWS), f32),
            ((2, 128, 128), f32),
            ((ROWS,), jnp.int32),
            ((1,), jnp.int32),
        ],
        copies=5 + LATER,
    )(
        far(me), far(doc_ids), far(log_step), far(log_extra.T), far(in_mix.reshape(2, 128, 128)),
        *map(far, later),
    )
    mixer_in, read_mix, skip_gain, out_weight, residual, routes, route_weight, norm_gain = map(
        near, later
    )
    messages = near(rows_exchanged(message))
    (partial,) = call(
        mixer_body,
        [VMEM] * 10,
        [((PEERS, ROWS, 128), bf16)],
        [
            ((2, tall, 128), f32),
            ((tall, 128), f32),
            ((BLOCKS * LINES, 128), f32),
            ((BLOCKS * GROUPS, 256), f32),
        ],
    )(
        messages, near(real), near(imag), near(keep), near(turn), near(span),
        mixer_in, read_mix, skip_gain, out_weight,
    )
    shares = near(exchanged(partial, TP))
    stream, outgoing = call(
        stream_body,
        [VMEM] * 3,
        [((ROWS, 128), bf16), ((BLOCKS * PAD, 128), bf16)],
    )(shares, residual, routes)
    arrived = rows_exchanged(outgoing)
    (copies,) = call(copies_body, [VMEM] * 2, [((PEERS // 2, 2 * SENT, 128), bf16)])(
        near(arrived), norm_gain
    )
    gathered = exchanged(copies.reshape(PEERS, SENT // 2, 2, 128), TP).reshape(copies.shape)
    (terms,) = call(
        expert_body,
        [VMEM] * 4,
        [((PEERS, EROWS, 128), bf16)],
        [((EROWS, 128 * PEERS), bf16), ((PEERS // 2, 2 * SENT, 128), f32)],
    )(near(gathered), switch_matrices, up_weight, down_weight)
    (answer,) = call(answer_body, [VMEM], [((BLOCKS * PAD, 128), bf16)])(
        near(exchanged(terms, TP))
    )
    returned = rows_exchanged(answer)
    (out,) = call(mixture_body, [VMEM] * 4, [((ROWS, 128), bf16)], last=True)(
        near(returned), near(stream), routes, route_weight
    )
    return out


def solution(mesh):
    split = Mesh(mesh.devices.reshape(mesh.shape["sp"], 4, 4), ("sp", "tp_0", "tp_1"))
    in_specs = (
        P("sp", TP),
        P("sp", TP),
        P("sp"),
        P(None, TP),
        P("sp", TP),
        P(None, TP, None, None),
        P(None, TP, None, None),
        P(TP),
        P(TP, None),
        P(TP),
        P("sp", None),
        P("sp", None),
        P("sp", None, TP),
        P("sp", None, TP),
        P("sp", TP, None),
    )
    out_specs = P("sp", TP)
    return jax.shard_map(
        shards, mesh=split, in_specs=in_specs, out_specs=out_specs, check_vma=False
    )
```

```python
import jax
import jax.numpy as jnp
from jax import lax
from jax.experimental import pallas as pl
from jax.experimental.pallas import tpu as pltpu
from jax.sharding import Mesh
from jax.sharding import PartitionSpec as P

TP = ("tp_0", "tp_1")
INTERPRET = False

epsilon = 1e-06
f32 = jnp.float32
bf16 = jnp.bfloat16

BLOCKS = 32
PEERS = 16
ROWS = 64
GROUPS = 8
SLOTS = 5
PAD = 6
LINES = 10
SPANS = 4
SQUARED = 4
LATER = 8
EROWS = BLOCKS * SLOTS
SENT = EROWS + 4

VMEM = pl.BlockSpec(memory_space=pltpu.VMEM)
SMEM = pl.BlockSpec(memory_space=pltpu.SMEM)
FAR = pl.BlockSpec(memory_space=pl.ANY if INTERPRET else pltpu.HBM)


def near(x):
    return x if INTERPRET else pltpu.with_memory_space_constraint(x, pltpu.VMEM)


def far(x):
    return x if INTERPRET else pltpu.with_memory_space_constraint(x, pltpu.HBM)


def call(body, in_specs, outs, scratch=(), copies=0, last=False):
    kept = jax.ShapeDtypeStruct if INTERPRET or last else pltpu.VMEM
    return pl.pallas_call(
        body,
        in_specs=in_specs,
        out_specs=[VMEM] * len(outs),
        out_shape=[kept(shape, dtype) for shape, dtype in outs],
        scratch_shapes=[
            (pltpu.SMEM if dtype == jnp.int32 else pltpu.VMEM)(shape, dtype)
            for shape, dtype in scratch
        ]
        + ([pltpu.SemaphoreType.DMA((copies,))] if copies else []),
        compiler_params=pltpu.CompilerParams(vmem_limit_bytes=16 * 2**20),
        interpret=INTERPRET,
    )


def iota(shape, dim):
    return lax.broadcasted_iota(jnp.int32, shape, dim)


def divided(x, by):
    return (x * (65536 // by + 1)) >> 16


def mm(a, b):
    return jnp.dot(a, b, preferred_element_type=f32)


def mm_across(a, b):
    return lax.dot_general(a, b, (((1,), (1,)), ((), ())), preferred_element_type=f32)


def halves_joined(first, second):
    left = iota((128, 128), 1) < 64
    return (
        jnp.where(left, first, pltpu.roll(second, 64, 1)),
        jnp.where(left, pltpu.roll(first, 64, 1), second),
    )


def steps_by_lane(log_step):
    eye = iota((GROUPS, GROUPS), 0) == iota((GROUPS, GROUPS), 1)
    step = jnp.exp(log_step)
    columns = [
        jnp.sum(
            jnp.where(eye, jnp.broadcast_to(step[k : k + 1, :], (GROUPS, GROUPS)), 0.0),
            axis=1,
            keepdims=True,
        )
        for k in range(2)
    ]
    return jnp.where(iota((GROUPS, 128), 1) < 64, columns[0], columns[1])


def turned(by_cos, by_sin, real, imag, new_real, new_imag):
    return (
        (by_cos * real + new_real) - by_sin * imag,
        (by_sin * real + new_imag) + by_cos * imag,
    )


def raised(cos, sin, squarings):
    for _ in range(squarings):
        cos, sin = cos * cos - sin * sin, 2.0 * cos * sin
    return cos, sin


def one_minus_exp(x):
    series = jnp.ones_like(x)
    for n in range(9, 1, -1):
        series = 1.0 - x * (1.0 / n) * series
    return jnp.where(x < 0.5, x * series, 1.0 - jnp.exp(-x))


def sweep_body(
    me_ref, far_docs, far_step, far_extra, far_mix, *refs
):
    far_later, refs = refs[:LATER], refs[LATER:]
    message_ref, real_ref, imag_ref, keep_ref, turn_ref, span_ref = refs[:6]
    later, refs = refs[6 : 6 + LATER], refs[6 + LATER :]
    masked, source, magnitude, log_step_ref, log_extra_ref, in_mix_ref, docs_ref, arrivals = refs
    x_ref = later[0]
    pairs = [
        (far_step, log_step_ref),
        (far_extra, log_extra_ref),
        (far_docs, docs_ref),
        (far_later[0], x_ref),
        (far_mix, in_mix_ref),
        *zip(far_later[1:], later[1:]),
    ]
    fetches = [
        pltpu.make_async_copy(distant, local, arrivals.at[k])
        for k, (distant, local) in enumerate(pairs)
    ]
    for fetch in fetches:
        fetch.start()
    for fetch in fetches[:5]:
        fetch.wait()
    lane = iota((GROUPS, 128), 1)
    fwd = lane < 64
    step = steps_by_lane(log_step_ref[...])
    theta = (jnp.pi * (lane & 63).astype(f32)) * step
    cos, sin = jnp.cos(theta), jnp.sin(theta)
    turn_ref[0] = cos
    turn_ref[1] = sin
    scale = jnp.sqrt(one_minus_exp(step))
    log_extra = log_extra_ref[...]
    loss = -0.5 * step
    for n in range(ROWS):
        extra = jnp.broadcast_to(log_extra[:, n : n + 1], (GROUPS, 128))
        magnitude[pl.ds(GROUPS * n, GROUPS), :] = jnp.exp(loss + extra)
    wide = iota((ROWS, 128), 1)
    x = x_ref[...].astype(f32)
    for g in range(GROUPS):
        masked[pl.ds(g, ROWS, stride=GROUPS), :] = jnp.where(wide // 16 == g, x, 0.0)
    mix_real, mix_imag = halves_joined(in_mix_ref[0], in_mix_ref[1])
    scales = jnp.concatenate(
        [jnp.broadcast_to(scale[g : g + 1, :], (16, 128)) for g in range(GROUPS)], axis=0
    )
    mix_real, mix_imag = mix_real * scales, mix_imag * scales
    rows = masked[...].astype(bf16)
    source[0] = mm(rows, mix_real.astype(bf16))
    source[1] = mm(rows, mix_imag.astype(bf16))
    real = jnp.zeros((GROUPS, 128), f32)
    imag = jnp.zeros((GROUPS, 128), f32)
    total = jnp.ones((GROUPS, 128), f32)
    for n in range(ROWS):
        r = ROWS - 1 - n
        here, there = pl.ds(GROUPS * n, GROUPS), pl.ds(GROUPS * r, GROUPS)
        keep = jnp.where(fwd, magnitude[here, :], magnitude[there, :])
        if n > 0:
            same_fwd = jnp.where(docs_ref[n] == docs_ref[n - 1], 1.0, 0.0)
            same_bwd = jnp.where(docs_ref[r] == docs_ref[r + 1], 1.0, 0.0)
            keep = keep * jnp.where(fwd, same_fwd, same_bwd)
        new_real = jnp.where(fwd, source[0, here, :], source[0, there, :])
        new_imag = jnp.where(fwd, source[1, here, :], source[1, there, :])
        keep_ref[n] = keep
        real_ref[n] = new_real
        imag_ref[n] = new_imag
        by_cos, by_sin = keep * cos, keep * sin
        real, imag = (
            (by_cos * real + new_real) - by_sin * imag,
            (by_sin * real + new_imag) + by_cos * imag,
        )
        total = total * keep
        if (n + 1) % (ROWS // SPANS) == 0 and n + 1 < ROWS:
            for k, reached in enumerate((real, imag, total)):
                span_ref[n // (ROWS // SPANS), k] = reached
    high = total.astype(bf16).astype(f32)
    low = total - high
    first_doc = docs_ref[0].astype(f32)
    last_doc = docs_ref[ROWS - 1].astype(f32)
    turn_ref[2] = jnp.where(fwd, first_doc, last_doc)
    group = iota((GROUPS, 128), 0)
    lines = []
    for kept, doc, left, right in [
        (0, last_doc, real, pltpu.roll(imag, 64, 1)),
        (64, first_doc, pltpu.roll(imag, 64, 1), real),
    ]:
        decays = jnp.where(lane == kept + group, high, 0.0) + jnp.where(
            lane == kept + GROUPS + group, low, 0.0
        )
        row = jnp.sum(decays, axis=0, keepdims=True) + jnp.where(
            lane[0:1] == kept + 2 * GROUPS, doc, 0.0
        )
        lines.append(jnp.where(fwd, left, right))
        lines.append(jnp.broadcast_to(row, (GROUPS, 128)))
    lines = jnp.concatenate(lines, axis=0).astype(bf16)
    row, entry = iota((BLOCKS * LINES, 32), 0), iota((BLOCKS * LINES, 32), 1)
    receiver = divided(row, LINES)
    wanted = row - receiver * LINES + jnp.where(receiver > me_ref[0], 0, 16)
    message_ref[...] = mm((entry == wanted).astype(f32).astype(bf16), lines).astype(bf16)
    for fetch in fetches[5:]:
        fetch.wait()


def mixer_body(
    me_ref, messages_ref, real_ref, imag_ref, keep_ref, turn_ref, span_ref,
    x_ref, read_mix_ref, skip_ref, out_weight_ref,
    partial_ref,
    states, read_out, received, spread,
):
    lane = iota((GROUPS, 128), 1)
    fwd = lane < 64
    me = me_ref[0]
    cos, sin, mine = turn_ref[0], turn_ref[1], turn_ref[2]
    span_cos, span_sin = raised(cos, sin, SQUARED)
    block_cos, block_sin = raised(span_cos, span_sin, 6 - SQUARED)
    received[...] = messages_ref[...].astype(f32)
    place, group = lane & 63, iota((GROUPS, 128), 0)
    of_group = (place == group) | (place == GROUPS + group) | (place == 2 * GROUPS)
    scalars = jnp.concatenate(
        [
            jnp.where(of_group, received[LINES * n + GROUPS : LINES * n + GROUPS + 1, :], 0.0)
            for n in range(BLOCKS)
        ],
        axis=0,
    ).astype(bf16)
    entry = iota((128, 256), 0) & 63
    left = iota((128, 256), 1) < 128
    summed = (left & (entry < 2 * GROUPS)) | (~left & (entry == 2 * GROUPS))
    spread[...] = mm(scalars, summed.astype(f32).astype(bf16))
    real = jnp.zeros((GROUPS, 128), f32)
    imag = jnp.zeros((GROUPS, 128), f32)
    for n in range(BLOCKS - 1):
        r = BLOCKS - 1 - n
        one = received[LINES * n : LINES * n + GROUPS, :]
        two = received[LINES * r : LINES * r + GROUPS, :]
        here, there = pl.ds(GROUPS * n, GROUPS), pl.ds(GROUPS * r, GROUPS)
        decay = jnp.where(fwd, spread[here, 0:128], spread[there, 0:128])
        same = jnp.where(fwd, spread[here, 128:256], spread[there, 128:256]) == mine
        new_real = jnp.where(same, jnp.where(fwd, one, two), 0.0)
        new_imag = jnp.where(same, pltpu.roll(jnp.where(fwd, two, one), 64, 1), 0.0)
        by_cos, by_sin = decay * block_cos, decay * block_sin
        passed = jnp.where(fwd, (n < me).astype(jnp.int32), (r > me).astype(jnp.int32)) > 0
        real, imag = (
            jnp.where(passed, (by_cos * real + new_real) - by_sin * imag, real),
            jnp.where(passed, (by_sin * real + new_imag) + by_cos * imag, imag),
        )
    span = ROWS // SPANS
    parts = [(real, imag)]
    far_cos, far_sin = span_cos, span_sin
    for q in range(SPANS - 1):
        total = span_ref[q, 2]
        parts.append(
            turned(total * far_cos, total * far_sin, real, imag, span_ref[q, 0], span_ref[q, 1])
        )
        far_cos, far_sin = (
            far_cos * span_cos - far_sin * span_sin,
            far_cos * span_sin + far_sin * span_cos,
        )
    for m in range(span):
        for q in range(SPANS):
            n = span * q + m
            r = ROWS - 1 - n
            here, there = pl.ds(GROUPS * n, GROUPS), pl.ds(GROUPS * r, GROUPS)
            keep = keep_ref[n]
            parts[q] = turned(keep * cos, keep * sin, *parts[q], real_ref[n], imag_ref[n])
            states[0, here, 0:64] = parts[q][0][:, 0:64]
            states[0, there, 64:128] = parts[q][0][:, 64:128]
            states[1, here, 0:64] = parts[q][1][:, 0:64]
            states[1, there, 64:128] = parts[q][1][:, 64:128]
    read_real, read_imag = halves_joined(read_mix_ref[0], read_mix_ref[1])
    read_out[...] = mm_across(states[0].astype(bf16), read_real.astype(bf16)) + mm_across(
        states[1].astype(bf16), read_imag.astype(bf16)
    )
    wide = iota((ROWS, 128), 1)
    mixed = skip_ref[...] * x_ref[...].astype(f32)
    for g in range(GROUPS):
        mixed = mixed + jnp.where(
            wide // 16 == g, read_out[pl.ds(g, ROWS, stride=GROUPS), :], 0.0
        )
    activated = jax.nn.gelu(mixed).astype(bf16)
    partial = mm(activated, out_weight_ref[...]).astype(bf16)
    for j in range(PEERS):
        partial_ref[j] = partial[:, 128 * j : 128 * (j + 1)]


def column(row):
    eye = iota((ROWS, ROWS), 0) == iota((ROWS, ROWS), 1)
    return jnp.sum(jnp.where(eye, row, 0.0), axis=1, keepdims=True)


def slots_down(routes, k):
    before = iota((ROWS, ROWS), 1) < iota((ROWS, ROWS), 0)
    expert = column(routes[k : k + 1])
    met = (expert == routes[0:1]).astype(f32) + (expert == routes[1:2]).astype(f32)
    rank = jnp.sum(jnp.where(before, met, 0.0), axis=1, keepdims=True)
    return expert * PAD + rank


def slots_across(routes, k):
    before = iota((ROWS, ROWS), 0) < iota((ROWS, ROWS), 1)
    expert = routes[k : k + 1]
    met = (column(routes[0:1]) == expert).astype(f32) + (column(routes[1:2]) == expert).astype(f32)
    rank = jnp.sum(jnp.where(before, met, 0.0), axis=0, keepdims=True)
    return expert * PAD + rank


def stream_body(arrived_ref, residual_ref, routes_ref, stream_ref, outgoing_ref):
    total = residual_ref[...].astype(f32)
    projected = arrived_ref[0].astype(f32)
    for j in range(1, PEERS):
        projected = projected + arrived_ref[j].astype(f32)
    stream = (total + projected).astype(bf16)
    stream_ref[...] = stream
    routes = routes_ref[...].astype(f32)
    slot = iota((BLOCKS * PAD, ROWS), 0).astype(f32)
    placing = (slot == slots_across(routes, 0)).astype(f32) + (
        slot == slots_across(routes, 1)
    ).astype(f32)
    outgoing_ref[...] = mm(placing.astype(bf16), stream).astype(bf16)


def packed_rows(shape, packed_dim):
    packed, padded = iota(shape, packed_dim), iota(shape, 1 - packed_dim)
    block = divided(padded, PAD)
    slot = padded - block * PAD
    return ((slot < SLOTS) & (packed == block * SLOTS + slot)).astype(f32).astype(bf16)


def copies_body(arrived_ref, gain_ref, copies_ref):
    row = iota((2 * SENT, BLOCKS * PAD), 0)
    row = jnp.where(row >= SENT, row - SENT, row)
    padded = iota((2 * SENT, BLOCKS * PAD), 1)
    block = divided(padded, PAD)
    slot = padded - block * PAD
    packing = (slot < SLOTS) & (row == block * SLOTS + slot)
    rows = mm(packing.astype(f32).astype(bf16), arrived_ref[...])
    gain = gain_ref[...]
    high = gain.astype(bf16).astype(f32)
    middle = (gain - high).astype(bf16).astype(f32)
    low = gain - high - middle
    row = iota((2 * SENT, 128), 0)
    row = jnp.where(row >= SENT, row - SENT, row) - EROWS
    for k, part in enumerate((high, middle, low)):
        rows = jnp.where(row == k, part, rows)
    rows = rows.astype(bf16)
    for j in range(PEERS // 2):
        copies_ref[j] = rows


def expert_body(rows_ref, gate_ref, up_ref, down_ref, terms_ref, normed, pieces):
    squares = jnp.zeros((EROWS, 128), f32)
    for j in range(PEERS // 2):
        pieces[j] = rows_ref[j].astype(f32)
    starts = [(j // 2, SENT * (j % 2)) for j in range(PEERS)]
    for block, start in starts:
        piece = pieces[block, start : start + EROWS, :]
        squares = squares + piece * piece
    mean = jnp.sum(squares, axis=1, keepdims=True) / (128 * PEERS)
    factor = lax.rsqrt(mean + epsilon)
    for j, (block, start) in enumerate(starts):
        end = start + EROWS
        gain = (
            pieces[block, end : end + 1, :]
            + pieces[block, end + 1 : end + 2, :]
            + pieces[block, end + 2 : end + 3, :]
        )
        piece = pieces[block, start:end, :]
        normed[:, 128 * j : 128 * (j + 1)] = (piece * factor * gain).astype(bf16)
    rows = normed[...]
    gate = mm(rows, gate_ref[0])
    up = mm(rows, up_ref[0])
    hidden = (jax.nn.silu(gate) * up).astype(bf16)
    terms = mm(hidden, down_ref[0]).astype(bf16)
    for j in range(PEERS):
        terms_ref[j] = terms[:, 128 * j : 128 * (j + 1)]


def answer_body(terms_ref, answer_ref):
    total = terms_ref[0].astype(f32)
    for j in range(1, PEERS):
        total = total + terms_ref[j].astype(f32)
    answer_ref[...] = mm(packed_rows((BLOCKS * PAD, EROWS), 1), total.astype(bf16)).astype(bf16)


def mixture_body(returned_ref, stream_ref, routes_ref, weight_ref, out_ref):
    routes, returned = routes_ref[...].astype(f32), returned_ref[...]
    slot = iota((ROWS, BLOCKS * PAD), 1).astype(f32)
    mixture = jnp.zeros((ROWS, 128), f32)
    for k in range(2):
        pick = (slot == slots_down(routes, k)).astype(f32).astype(bf16)
        mixture = mixture + mm(pick, returned) * column(weight_ref[k : k + 1, :])
    out_ref[...] = (stream_ref[...].astype(f32) + mixture).astype(bf16)


def exchanged(pieces, axis):
    return lax.all_to_all(pieces, axis, 0, 0, tiled=True)


def rows_exchanged(rows):
    pairs = rows.reshape(BLOCKS, rows.shape[0] // (2 * BLOCKS), 2, rows.shape[1])
    return exchanged(pairs, "sp").reshape(rows.shape)


def shards(
    mixer_in,
    residual,
    doc_ids,
    log_step,
    log_extra,
    in_mix,
    read_mix,
    skip_gain,
    out_weight,
    norm_gain,
    routes,
    route_weight,
    switch_matrices,
    up_weight,
    down_weight,
):
    me = lax.axis_index("sp").reshape(1)
    tall = GROUPS * ROWS
    later = (
        mixer_in,
        read_mix.swapaxes(2, 3).reshape(2, 128, 128),
        skip_gain.reshape(1, 128),
        out_weight,
        residual,
        routes.T,
        route_weight.T,
        norm_gain.reshape(1, 128),
    )
    message, real, imag, keep, turn, span, *later = call(
        sweep_body,
        [SMEM] + [FAR] * (4 + LATER),
        [
            ((BLOCKS * LINES, 128), bf16),
            ((ROWS, GROUPS, 128), f32),
            ((ROWS, GROUPS, 128), f32),
            ((ROWS, GROUPS, 128), f32),
            ((3, GROUPS, 128), f32),
            ((SPANS - 1, 3, GROUPS, 128), f32),
            *((x.shape, x.dtype) for x in later),
        ],
        [
            ((tall, 128), f32),
            ((2, tall, 128), f32),
            ((tall, 128), f32),
            ((2, GROUPS), f32),
            ((GROUPS, ROWS), f32),
            ((2, 128, 128), f32),
            ((ROWS,), jnp.int32),
        ],
        copies=4 + LATER,
    )(
        me, far(doc_ids), far(log_step), far(log_extra.T), far(in_mix.reshape(2, 128, 128)),
        *map(far, later),
    )
    mixer_in, read_mix, skip_gain, out_weight, residual, routes, route_weight, norm_gain = map(
        near, later
    )
    messages = near(rows_exchanged(message))
    (partial,) = call(
        mixer_body,
        [SMEM] + [VMEM] * 10,
        [((PEERS, ROWS, 128), bf16)],
        [
            ((2, tall, 128), f32),
            ((tall, 128), f32),
            ((BLOCKS * LINES, 128), f32),
            ((BLOCKS * GROUPS, 256), f32),
        ],
    )(
        me, messages, near(real), near(imag), near(keep), near(turn), near(span),
        mixer_in, read_mix, skip_gain, out_weight,
    )
    shares = near(exchanged(partial, TP))
    stream, outgoing = call(
        stream_body,
        [VMEM] * 3,
        [((ROWS, 128), bf16), ((BLOCKS * PAD, 128), bf16)],
    )(shares, residual, routes)
    arrived = rows_exchanged(outgoing)
    (copies,) = call(copies_body, [VMEM] * 2, [((PEERS // 2, 2 * SENT, 128), bf16)])(
        near(arrived), norm_gain
    )
    gathered = exchanged(copies.reshape(PEERS, SENT // 2, 2, 128), TP).reshape(copies.shape)
    (terms,) = call(
        expert_body,
        [VMEM] * 4,
        [((PEERS, EROWS, 128), bf16)],
        [((EROWS, 128 * PEERS), bf16), ((PEERS // 2, 2 * SENT, 128), f32)],
    )(near(gathered), switch_matrices, up_weight, down_weight)
    (answer,) = call(answer_body, [VMEM], [((BLOCKS * PAD, 128), bf16)])(
        near(exchanged(terms, TP))
    )
    returned = rows_exchanged(answer)
    (out,) = call(mixture_body, [VMEM] * 4, [((ROWS, 128), bf16)], last=True)(
        near(returned), near(stream), routes, route_weight
    )
    return out


def solution(mesh):
    split = Mesh(mesh.devices.reshape(mesh.shape["sp"], 4, 4), ("sp", "tp_0", "tp_1"))
    in_specs = (
        P("sp", TP),
        P("sp", TP),
        P("sp"),
        P(None, TP),
        P("sp", TP),
        P(None, TP, None, None),
        P(None, TP, None, None),
        P(TP),
        P(TP, None),
        P(TP),
        P("sp", None),
        P("sp", None),
        P("sp", None, TP),
        P("sp", None, TP),
        P("sp", TP, None),
    )
    out_specs = P("sp", TP)
    return jax.shard_map(
        shards, mesh=split, in_specs=in_specs, out_specs=out_specs, check_vma=False
    )
```
